128 devices in a mesh: sp: 64 (over z, y, x), tp: 2 (over core).
Axes of the slice: x: 4, y: 4, z: 4, core: 2. Of those that a mesh axis runs over, the one named last changes fastest.
Arguments:
- mid_rows: bfloat16 [8192, 2048], P(('sp', 'tp')), may hold values from -6 to 6
- cotangent: bfloat16 [8192, 2048], P(('sp', 'tp')), may hold values from -24 to 24
- route_experts: int32 [8192, 2], P(('sp', 'tp')), may hold values from 0 to 63, as said below
- route_weights: float32 [8192, 2], P(('sp', 'tp')), may hold values from 0.05 to 0.6
- gate_weight: bfloat16 [64, 2048, 1024], P('sp', None, 'tp'), may hold values from -0.125 to 0.125
- up_weight: bfloat16 [64, 2048, 1024], P('sp', None, 'tp'), may hold values from -0.125 to 0.125
- down_weight: bfloat16 [64, 1024, 2048], P('sp', 'tp'), may hold values from -0.1875 to 0.1875
- out_weight: bfloat16 [2048, 2048], P(None, 'tp'), may hold values from -0.125 to 0.125
- queries: bfloat16 [8192, 1024], P('sp', 'tp'), may hold values from -6 to 6
- key_rows: bfloat16 [8192, 1024], P('sp', 'tp'), may hold values from -6 to 6
- value_rows: bfloat16 [8192, 2048], P('sp', 'tp'), may hold values from -6 to 6
- log_decay: float32 [8192, 1024], P('sp', 'tp'), may hold values from -1 to 0
Outputs:
- gate_gradient: bfloat16 [64, 2048, 1024], P('sp', None, 'tp')
- up_gradient: bfloat16 [64, 2048, 1024], P('sp', None, 'tp')
- down_gradient: bfloat16 [64, 1024, 2048], P('sp', 'tp')
- out_gradient: float32 [2048, 2048], P('sp', 'tp')
- query_gradient: bfloat16 [8192, 1024], P('sp', 'tp')
- key_gradient: bfloat16 [8192, 1024], P('sp', 'tp')
- value_gradient: bfloat16 [8192, 2048], P('sp', 'tp')
- decay_gradient: float32 [8192, 1024], P('sp', 'tp')
The draws below stay inside these ranges and needn't reach their ends.
Inputs may be any that keep to these rules, and one draw needn't show every extreme that they name: `route_experts`: each row names two different experts of one group: both lie among the same 16 consecutive numbers starting at a multiple of 16. Among the rows of one device, no expert is named more than 4 times, and one expert exactly 4 times.
All inputs are finite; a program needn't handle non-finite values.
Results may differ from the reference program's by a relative error of at most 0.0058.
Values may be sent and summed in bfloat16 or wider, within the bound.
A program may use at most 192 MiB of HBM per device.

```python
import math
import jax
import jax.numpy as jnp
from jax import lax

D = 2048
HEADS = 8
DK = 128
DV = 256
KEY_CHANNELS = 1024
VW = 2048
DE = 1024
GROUPS = 4
BLOCK = 64
TOK_DEV = 128
SEQUENCE_TOKENS = 8192
ROWS = 64
EXPERTS = 64
CAP = 4


def route_block(block_key):
    per_group = EXPERTS // GROUPS
    half_rows = ROWS // 2
    first_key, second_key, third_key, fourth_key = jax.random.split(block_key, 4)
    token_position = jnp.arange(ROWS, dtype=jnp.int32)
    heavy = token_position < half_rows
    cut_points = jax.random.randint(fourth_key, (2,), 0, half_rows + 1).astype(jnp.int32)
    lower_cut = jnp.minimum(cut_points[0], cut_points[1])
    upper_cut = jnp.maximum(cut_points[0], cut_points[1])
    spare = token_position - half_rows
    other_group = jnp.where(spare < lower_cut, 1, jnp.where(spare < upper_cut, 2, 3)).astype(jnp.int32)
    other_start = jnp.where(other_group == 1, 0, jnp.where(other_group == 2, lower_cut, upper_cut)).astype(jnp.int32)
    group = jnp.where(heavy, 0, other_group).astype(jnp.int32)
    group_rank = jnp.where(heavy, token_position, spare - other_start).astype(jnp.int32)
    local_first = group_rank % per_group
    local_second = (group_rank + 1) % per_group
    group_order = jax.random.permutation(first_key, GROUPS).astype(jnp.int32)
    local_keys = jax.random.split(second_key, GROUPS)
    local_order = jax.vmap(jax.random.permutation, in_axes=(0, None))(local_keys, per_group).astype(jnp.int32)
    target = group_order[group]
    expert_first = target * per_group + local_order[group, local_first]
    expert_second = target * per_group + local_order[group, local_second]
    paired = jnp.stack([expert_first, expert_second], axis=1)
    shuffle = jax.random.permutation(third_key, ROWS)
    return paired[shuffle].astype(jnp.int32)


def draw_route_experts(key, part):
    block_total = SEQUENCE_TOKENS // ROWS
    block_keys = jax.random.split(jax.random.fold_in(key, 11), block_total)
    return jax.vmap(route_block)(block_keys).reshape(SEQUENCE_TOKENS, 2).astype(jnp.int32)


def draw_log_decay(key, part):
    random_subkeys = jax.random.split(jax.random.fold_in(key, 23), 7)
    fast_share = 0.5
    fast_channel = jax.random.bernoulli(random_subkeys[0], fast_share, (KEY_CHANNELS,))
    slow_rate = jnp.exp(jax.random.uniform(random_subkeys[1], (KEY_CHANNELS,), jnp.float32, jnp.log(0.1), 0.0)) * (0.5 / SEQUENCE_TOKENS)
    fast_rate = jax.random.uniform(random_subkeys[2], (KEY_CHANNELS,), jnp.float32, 0.01, 1.0 / 30.0)
    channel_decay_rate = jnp.where(fast_channel, fast_rate, slow_rate)
    device_multiplier = jnp.exp(jax.random.uniform(random_subkeys[3], (SEQUENCE_TOKENS // TOK_DEV,), jnp.float32, jnp.log(0.5), 0.0))
    device_multiplier = jnp.repeat(device_multiplier, TOK_DEV)
    random_noise = jax.random.uniform(random_subkeys[4], (SEQUENCE_TOKENS, KEY_CHANNELS), jnp.float32, 0.5, 1.5)
    spike_location = jax.random.randint(random_subkeys[5], (2,), 0, SEQUENCE_TOKENS)
    spike_magnitude = jax.random.uniform(random_subkeys[6], (2, KEY_CHANNELS), jnp.float32, jnp.log(0.5), jnp.log(0.8))
    token_position = jnp.arange(SEQUENCE_TOKENS)
    spike_value = jnp.where(token_position[:, None] == spike_location[0], spike_magnitude[0][None, :], 0.0)
    spike_value = spike_value + jnp.where(token_position[:, None] == spike_location[1], spike_magnitude[1][None, :], 0.0)
    return (spike_value - channel_decay_rate[None, :] * device_multiplier[:, None] * random_noise).astype(jnp.float32)


def spiked(values, key, source, target, blocks, factor):
    def block_of(dim):
        return (jnp.arange(values.shape[dim]) // (values.shape[dim] // blocks)).reshape((-1,) + (1,) * (values.ndim - 1 - dim))

    one_side = jax.random.permutation(key, blocks)[block_of(target)]
    other_side = (block_of(target) + blocks // 2) % blocks
    return jnp.where((block_of(source) == one_side) | (block_of(source) == other_side), factor * values, values)


def levels(stream_key, shape, cuts, smallest, high):
    def one(position, parts):
        draws = jax.random.uniform(jax.random.fold_in(jax.random.fold_in(stream_key, 6), position), (parts,), jnp.float32, smallest / len(cuts), high / len(cuts))
        return jnp.repeat(jnp.exp(draws), shape[position] // parts).reshape((-1,) + (1,) * (len(shape) - position - 1))

    gain = one(*cuts[0])
    for cut in cuts[1:]:
        gain = gain * one(*cut)
    return gain


def gaussian(stream_key, shape, spread, reach, cuts=(), kind=jnp.bfloat16):
    values = jax.random.normal(stream_key, shape, jnp.float32) * spread
    if len(cuts) > 0:
        values = levels(stream_key, shape, cuts, -0.22, 0.18) * values
    return jnp.clip(values, min=-reach, max=reach).astype(kind)


def heavy_noise(own_key, dims, scale, bound, cuts, heavy, held_as=jnp.bfloat16):
    result = scale * jax.random.normal(own_key, dims, jnp.float32)
    if cuts:
        result = result * levels(own_key, dims, cuts, -0.22, 0.18)
    return jnp.clip(spiked(result, jax.random.fold_in(own_key, 3), *heavy), -bound, bound).astype(held_as)


def setup_inputs(seed: int = 0) -> dict:
    arg_keys = jax.random.split(jax.random.key(seed), 13)
    return {
        "mid_rows": gaussian(arg_keys[0], (SEQUENCE_TOKENS, D), 1.0, 6.0, ((0, 128),)),
        "cotangent": heavy_noise(arg_keys[1], (SEQUENCE_TOKENS, D), 1.0, 24.0, ((0, 128),), (0, 1, 128, 5.5)),
        "route_experts": draw_route_experts(jax.random.fold_in(arg_keys[12], 71), 0),
        "route_weights": jnp.clip(jnp.exp(math.log(0.6) - 2.4849067 * jax.random.uniform(arg_keys[3], (SEQUENCE_TOKENS, 2), jnp.float32) ** levels(arg_keys[3], (SEQUENCE_TOKENS, 2), ((0, 128),), -0.2, 0.2)), 0.05, 0.6),
        "gate_weight": gaussian(arg_keys[4], (EXPERTS, D, DE), D ** -0.5, 0.125, ((0, 64), (2, 2))),
        "up_weight": gaussian(arg_keys[5], (EXPERTS, D, DE), D ** -0.5, 0.125, ((0, 64), (2, 2))),
        "down_weight": gaussian(arg_keys[6], (EXPERTS, DE, D), DE ** -0.5, 0.1875, ((0, 64), (1, 2))),
        "out_weight": gaussian(arg_keys[7], (D, VW), VW ** -0.5, 0.125, ((1, 2),)),
        "queries": gaussian(arg_keys[8], (SEQUENCE_TOKENS, KEY_CHANNELS), 1.0, 6.0, ((0, 64), (1, 2))),
        "key_rows": gaussian(arg_keys[9], (SEQUENCE_TOKENS, KEY_CHANNELS), 1.0, 6.0, ((0, 64), (1, 2))),
        "value_rows": gaussian(arg_keys[10], (SEQUENCE_TOKENS, VW), 1.0, 6.0, ((0, 64), (1, 2))),
        "log_decay": draw_log_decay(jax.random.fold_in(arg_keys[12], 71), 0),
    }


precise = lax.Precision.HIGHEST
epsilon = 1e-06
contract_rows = (((0,), (0,)), ((), ()))
contract_cols = (((1,), (1,)), ((), ()))

def silu_parts(pre_gate):
    gate_sigmoid = jax.nn.sigmoid(pre_gate)
    gate_swish = pre_gate * gate_sigmoid
    gate_slope = gate_sigmoid * (1.0 + pre_gate * (1.0 - gate_sigmoid))
    return (gate_swish, gate_slope)

def mixer_normed(query_float, key_float, value_float, decay_float):
    block_count = SEQUENCE_TOKENS // BLOCK
    query_blocks = query_float.reshape(block_count, BLOCK, HEADS, DK) * DK ** (-0.5)
    key_blocks = key_float.reshape(block_count, BLOCK, HEADS, DK)
    value_blocks = value_float.reshape(block_count, BLOCK, HEADS, DV)
    decay_blocks = decay_float.reshape(block_count, BLOCK, HEADS, DK)
    lower_mask = jnp.tril(jnp.ones((BLOCK, BLOCK), jnp.float32))

    def advance(carry_state, inputs):
        query_block, key_block, value_block, decay_block = inputs
        running_log = jnp.cumsum(decay_block, axis=0)
        block_log = running_log[-1]
        query_decayed = query_block * jnp.exp(running_log)
        key_inverse = key_block * jnp.exp(-running_log)
        key_to_end = key_block * jnp.exp(block_log[None] - running_log)
        scores = jnp.einsum('ihc,jhc->hij', query_decayed, key_inverse, precision=precise) * lower_mask
        raw_out = jnp.einsum('hij,jhv->ihv', scores, value_block, precision=precise)
        raw_out = raw_out + jnp.einsum('ihc,hcv->ihv', query_decayed, carry_state, precision=precise)
        new_state = jnp.exp(block_log)[:, :, None] * carry_state + jnp.einsum('jhc,jhv->hcv', key_to_end, value_block, precision=precise)
        return (new_state, raw_out)
    zero_state = jnp.zeros((HEADS, DK, DV), jnp.float32)
    final_state, raw_out = lax.scan(advance, zero_state, (query_blocks, key_blocks, value_blocks, decay_blocks))
    inverse_root = lax.rsqrt(lax.optimization_barrier(jnp.mean(raw_out * raw_out, axis=-1, keepdims=True)) + epsilon)
    return (raw_out * inverse_root).reshape(SEQUENCE_TOKENS, HEADS * DV)

def reference(mid_rows, cotangent, route_experts, route_weights, gate_weight, up_weight, down_weight, out_weight, queries, key_rows, value_rows, log_decay):
    senders = SEQUENCE_TOKENS // ROWS
    slots_total = senders * CAP
    sender_picks = route_experts.reshape(senders, 2 * ROWS)
    one_hot = (sender_picks[:, :, None] == jnp.arange(EXPERTS, dtype=jnp.int32)[None, None, :]).astype(jnp.int32)
    slot_rank = lax.optimization_barrier(jnp.sum((jnp.cumsum(one_hot, axis=1) - one_hot) * one_hot, axis=2))
    slot_index = (jnp.arange(senders, dtype=jnp.int32)[:, None] * CAP + slot_rank).reshape(-1).astype(jnp.int32)
    flat_expert = sender_picks.reshape(-1)
    table = jnp.full((EXPERTS, slots_total), -1, jnp.int32).at[flat_expert, slot_index].set(jnp.arange(2 * SEQUENCE_TOKENS, dtype=jnp.int32))
    flat_weight = route_weights.reshape(-1)
    half_width = DE // 2

    def one_expert(inputs):
        gate_expert, up_expert, down_expert, entries = inputs
        live_slot = entries >= 0
        entry_index = jnp.maximum(entries, 0)
        token_index = entry_index // 2
        rows_in = jnp.where(live_slot[:, None], mid_rows[token_index], jnp.zeros((), jnp.bfloat16))
        scaled = jnp.where(live_slot[:, None], flat_weight[entry_index][:, None] * cotangent[token_index].astype(jnp.float32), 0.0).astype(jnp.bfloat16)
        pre_gate = jnp.dot(rows_in, gate_expert, preferred_element_type=jnp.float32)
        pre_up = jnp.dot(rows_in, up_expert, preferred_element_type=jnp.float32)
        gate_swish, gate_slope = silu_parts(pre_gate)
        hidden = (gate_swish * pre_up).astype(jnp.bfloat16)
        back_hidden = lax.dot_general(scaled, down_expert, contract_cols, preferred_element_type=jnp.float32)
        back_gate = (back_hidden * pre_up * gate_slope).astype(jnp.bfloat16)
        back_up = (back_hidden * gate_swish).astype(jnp.bfloat16)
        gate_total = lax.dot_general(rows_in, back_gate, contract_rows, preferred_element_type=jnp.float32).astype(jnp.bfloat16)
        up_total = lax.dot_general(rows_in, back_up, contract_rows, preferred_element_type=jnp.float32).astype(jnp.bfloat16)
        down_total = lax.dot_general(hidden, scaled, contract_rows, preferred_element_type=jnp.float32).astype(jnp.bfloat16)
        first_half = lax.dot_general(back_gate[:, :half_width], gate_expert[:, :half_width], contract_cols, preferred_element_type=jnp.float32)
        first_half = first_half + lax.dot_general(back_up[:, :half_width], up_expert[:, :half_width], contract_cols, preferred_element_type=jnp.float32)
        second_half = lax.dot_general(back_gate[:, half_width:], gate_expert[:, half_width:], contract_cols, preferred_element_type=jnp.float32)
        second_half = second_half + lax.dot_general(back_up[:, half_width:], up_expert[:, half_width:], contract_cols, preferred_element_type=jnp.float32)
        first_round, second_round = lax.optimization_barrier((first_half.astype(jnp.bfloat16), second_half.astype(jnp.bfloat16)))
        expert_rows = (first_round.astype(jnp.float32) + second_round.astype(jnp.float32)).astype(jnp.bfloat16)
        return (gate_total, up_total, down_total, expert_rows)
    gate_total, up_total, down_total, expert_rows = lax.map(one_expert, (gate_weight, up_weight, down_weight, table))
    picked = expert_rows[flat_expert, slot_index].reshape(SEQUENCE_TOKENS, 2, D)
    token_back = (cotangent.astype(jnp.float32) + picked[:, 0].astype(jnp.float32) + picked[:, 1].astype(jnp.float32)).astype(jnp.bfloat16)
    normed, pullback = jax.vjp(mixer_normed, queries.astype(jnp.float32), key_rows.astype(jnp.float32), value_rows.astype(jnp.float32), log_decay)
    normed_rows = normed.astype(jnp.bfloat16)
    out_gradient = lax.dot_general(token_back, normed_rows, contract_rows, preferred_element_type=jnp.float32)
    back_normed = jnp.dot(token_back, out_weight, preferred_element_type=jnp.float32)
    query_back, key_back, value_back, decay_back = pullback(back_normed)
    return (gate_total, up_total, down_total, out_gradient, query_back.astype(jnp.bfloat16), key_back.astype(jnp.bfloat16), value_back.astype(jnp.bfloat16), decay_back)
```

```python
import jax
import jax.numpy as jnp
from jax import lax
from jax.experimental import pallas as pl
from jax.experimental.pallas import tpu as pltpu
from jax.sharding import Mesh
from jax.sharding import PartitionSpec as P

DK = 128
DV = 256
BLOCK = 64
SP = ("sp_0", "sp_1", "sp_2")
SP_TP = ("sp_0", "sp_1", "sp_2", "tp")


precise = lax.Precision.HIGHEST
epsilon = 1e-06
contract_rows = (((0,), (0,)), ((), ()))
contract_cols = (((1,), (1,)), ((), ()))
MESH = pl.DeviceIdType.MESH


def in_blocks(shard, dim, count):
    before, after = (shard.shape[:dim], shard.shape[dim + 1 :])
    return jnp.moveaxis(shard.reshape(*before, count, -1, *after), dim, 0)


def summed_on_arrival(shard, axis, dim):
    blocks = in_blocks(shard, dim, lax.axis_size(axis))
    arrived = lax.all_to_all(blocks, axis, split_axis=0, concat_axis=0, tiled=True)
    return arrived.astype(jnp.float32).sum(axis=0)


def neutral_like(shard, identity):
    return jax.tree.map(
        lambda a, e: jnp.broadcast_to(jnp.asarray(e, a.dtype), a.shape), shard, identity
    )


def carried_in(shard, axes, combine, identity, reverse):
    before = start = neutral_like(shard, identity)
    subtotal = shard
    for axis in reversed(axes):
        count, here = (lax.axis_size(axis), lax.axis_index(axis))
        pieces = jax.tree.map(lambda part: lax.all_gather(part, axis), subtotal)
        inside, subtotal = (start, start)
        for k in reversed(range(count)) if reverse else range(count):
            passed = k > here if reverse else k < here
            subtotal = combine(subtotal, jax.tree.map(lambda part: part[k], pieces))
            inside = jax.tree.map(lambda new, old: jnp.where(passed, new, old), subtotal, inside)
        before = combine(inside, before)
    return before


def silu_parts(pre_gate):
    gate_sigmoid = jax.nn.sigmoid(pre_gate)
    gate_swish = pre_gate * gate_sigmoid
    gate_slope = gate_sigmoid * (1.0 + pre_gate * (1.0 - gate_sigmoid))
    return (gate_swish, gate_slope)


def ring(base, step):
    return lax.rem(base + step, 4)


def rows_at(start, size):
    return pl.ds(pl.multiple_of(start, size), size)


def dot(a, b):
    return lax.dot_general(a, b, (((1,), (0,)), ((), ())), preferred_element_type=jnp.float32)


def dot_rows(a, b):
    return lax.dot_general(a, b, contract_rows, preferred_element_type=jnp.float32)


def dot_cols(a, b):
    return lax.dot_general(a, b, contract_cols, preferred_element_type=jnp.float32)


def ones_where(mask):
    return jnp.where(mask, 1.0, 0.0).astype(jnp.float32)


def bf(a):
    return a.astype(jnp.bfloat16)


def pieces_of(a):
    high = bf(a).astype(jnp.float32)
    mid = bf(a - high).astype(jnp.float32)
    return high, mid, a - high - mid


PLANE = sorted(
    [(dy, dx) for dy in range(4) for dx in range(4) if (dy, dx) != (0, 0)],
    key=lambda o: -(min(o[0], 4 - o[0]) + min(o[1], 4 - o[1])),
)
CHUNKS = 2
WIDE = 2048 // CHUNKS


def expert_kernel(
    experts_ref,
    weights_ref,
    mid_ref,
    cot_ref,
    gate_hbm,
    up_hbm,
    down_hbm,
    token_ref,
    gate_out,
    up_out,
    down_out,
    gate_w,
    up_w,
    down_w,
    z_send,
    z_note_send,
    z_recv,
    z_note,
    x_send,
    rows,
    pre_gate,
    pre_up,
    back_hidden,
    hidden,
    back_gate,
    back_up,
    half_send,
    half_recv,
    own_half,
    ret_send,
    ret_recv,
    tok_send,
    tok_recv,
    token_all,
    grad_buf,
    w_sem,
    z_ss,
    z_rs,
    n_ss,
    n_rs,
    x_ss,
    x_rs,
    d_ss,
    d_rs,
    h_ss,
    h_rs,
    r_ss,
    r_rs,
    t_ss,
    t_rs,
    a_ss,
    a_rs,
    g_sem,
):
    z, y, x, tp = [lax.axis_index(a) for a in SP_TP]
    other = 1 - tp
    here = y * 4 + x
    mine = tp * 256

    def z_peer(dz):
        return (ring(z, dz), y, x, tp)

    def plane_peer(dy, dx):
        return (z, ring(y, dy), ring(x, dx), tp)

    partner = (z, y, x, other)
    barrier = pltpu.get_barrier_semaphore()
    peers = [z_peer(dz) for dz in (1, 2, 3)] + [plane_peer(*o) for o in PLANE] + [partner]
    for peer in peers:
        pl.semaphore_signal(barrier, inc=1, device_id=peer, device_id_type=MESH)

    loads = []
    for n, (src, dst) in enumerate(((gate_hbm, gate_w), (up_hbm, up_w), (down_hbm, down_w))):
        load = pltpu.make_async_copy(src.at[0], dst, w_sem.at[n])
        load.start()
        loads.append(load)

    def remote(src, dst, ss, rs, peer):
        copy = pltpu.make_async_remote_copy(
            src_ref=src, dst_ref=dst, send_sem=ss, recv_sem=rs, device_id=peer, device_id_type=MESH
        )
        copy.start()
        return copy

    sent = []

    lane = lax.broadcasted_iota(jnp.int32, (64, 128), 1)
    first = experts_ref[:, 0:1]
    second = experts_ref[:, 1:2]
    named_first = ones_where(lane == first)
    named_second = ones_where(lane == second)
    before = bf(
        ones_where(
            lax.broadcasted_iota(jnp.int32, (64, 64), 0)
            > lax.broadcasted_iota(jnp.int32, (64, 64), 1)
        )
    )
    counts = dot(before, bf(named_first + named_second))
    rank_first = jnp.sum(named_first * counts, axis=1, keepdims=True)
    rank_second = jnp.sum(named_second * counts, axis=1, keepdims=True)
    group = lax.shift_right_logical(first, 4)
    in_group = ones_where(lane == group)
    group_rank = jnp.sum(in_group * dot(before, bf(in_group)), axis=1, keepdims=True)
    z_slot = group * 32 + group_rank.astype(jnp.int32)
    z_pick = bf(ones_where(lane == z_slot))
    slot_first = (jnp.bitwise_and(first, 15) * 16).astype(jnp.float32) + rank_first
    slot_second = (jnp.bitwise_and(second, 15) * 16).astype(jnp.float32) + rank_second
    columns = [slot_first, slot_second]
    columns += list(pieces_of(weights_ref[:, 0:1])) + list(pieces_of(weights_ref[:, 1:2]))
    note = ones_where(lane == 8)
    for n, column in enumerate(columns):
        note = jnp.where(lane == n, column, note)
    z_note_send[...] = bf(dot_rows(z_pick, bf(note)))
    for c in range(CHUNKS):
        cut = slice(c * WIDE, (c + 1) * WIDE)
        z_send[c, :, :WIDE] = bf(dot_rows(z_pick, mid_ref[:, cut]))
        z_send[c, :, WIDE:] = bf(dot_rows(z_pick, cot_ref[:, cut]))

    pl.semaphore_wait(barrier, len(peers))

    z_copies = []
    note_copies = []
    for n, dz in enumerate((2, 1, 3)):
        there = rows_at(ring(z, dz) * 32, 32)
        note_copies.append(
            remote(
                z_note_send.at[there],
                z_note.at[rows_at(z * 32, 32)],
                n_ss.at[n],
                n_rs.at[n],
                z_peer(dz),
            )
        )
    for c in range(CHUNKS):
        z_copies.append([])
        for n, dz in enumerate((2, 1, 3)):
            there = rows_at(ring(z, dz) * 32, 32)
            z_copies[c].append(
                remote(
                    z_send.at[c, there],
                    z_recv.at[c, rows_at(z * 32, 32)],
                    z_ss.at[c, n],
                    z_rs.at[c, n],
                    z_peer(dz),
                )
            )
    own_z = rows_at(z * 32, 32)
    z_note[own_z, :] = z_note_send[own_z, :]
    for c in range(CHUNKS):
        z_recv[c, own_z, :] = z_send[c, own_z, :]

    for copy in note_copies:
        copy.wait_recv()
    got = z_note[...].astype(jnp.float32)
    token_row = lax.broadcasted_iota(jnp.int32, (128, 1), 0)
    offset = lax.shift_right_logical(token_row, 5) * 4
    live = got[:, 8:9] > 0.5
    slot_a = jnp.where(live, got[:, 0:1].astype(jnp.int32) + offset, -1)
    slot_b = jnp.where(live, got[:, 1:2].astype(jnp.int32) + offset, -1)
    slot_lane = lax.broadcasted_iota(jnp.int32, (128, 256), 1)
    place_a = bf(ones_where(slot_lane == slot_a))
    place_b = bf(ones_where(slot_lane == slot_b))
    place = place_a + place_b
    weight_a = got[:, 2:3] + got[:, 3:4] + got[:, 4:5]
    weight_b = got[:, 5:6] + got[:, 6:7] + got[:, 7:8]

    x_copies = []
    own_x = rows_at(here * 16, 16)
    for c in range(CHUNKS):
        for copy in z_copies[c]:
            copy.wait_recv()
        x_send[c, :, :WIDE] = bf(dot_rows(place, z_recv[c, :, :WIDE]))
        cot_part = z_recv[c, :, WIDE:].astype(jnp.float32)
        x_send[c, :, WIDE:] = bf(
            dot_rows(place_a, bf(weight_a * cot_part)) + dot_rows(place_b, bf(weight_b * cot_part))
        )
        x_copies.append([])
        for n, (dy, dx) in enumerate(PLANE):
            there = rows_at((ring(y, dy) * 4 + ring(x, dx)) * 16, 16)
            x_copies[c].append(
                remote(
                    x_send.at[c, there],
                    rows.at[c, rows_at(mine + here * 16, 16)],
                    x_ss.at[c, n],
                    x_rs.at[c, n],
                    plane_peer(dy, dx),
                )
            )
        rows[c, rows_at(mine + here * 16, 16), :] = x_send[c, own_x, :]

    for load in loads:
        load.wait()
    for c in range(CHUNKS):
        shares = []
        for n, (dy, dx) in enumerate(((0, 0),) + tuple(PLANE)):
            if n:
                x_copies[c][n - 1].wait_recv()
            source = ring(y, 4 - dy) * 4 + ring(x, 4 - dx)
            part = rows.at[c, rows_at(mine + source * 16, 16)]
            shares.append(remote(part, part, d_ss.at[c, n], d_rs.at[c, n], partner))
        for copy in shares:
            copy.wait_recv()
        sent += shares
        cut = slice(c * WIDE, (c + 1) * WIDE)
        for ref, weight in ((pre_gate, gate_w), (pre_up, up_w)):
            value = dot(rows[c, :, :WIDE], weight[cut, :])
            ref[...] = value if c == 0 else ref[...] + value
        value = dot_cols(rows[c, :, WIDE:], down_w[:, cut])
        back_hidden[...] = value if c == 0 else back_hidden[...] + value

    gate_swish, gate_slope = silu_parts(pre_gate[...])
    hidden[...] = bf(gate_swish * pre_up[...])
    back_gate[...] = bf(back_hidden[...] * pre_up[...] * gate_slope)
    back_up[...] = bf(back_hidden[...] * gate_swish)

    half_copies = []
    their_rows = rows_at(other * 256, 256)
    own_rows = rows_at(mine, 256)
    for c in range(CHUNKS):
        cut = slice(c * WIDE, (c + 1) * WIDE)
        half_send[c] = bf(
            dot_cols(back_gate[their_rows, :], gate_w[cut, :])
            + dot_cols(back_up[their_rows, :], up_w[cut, :])
        )
        half_copies.append(
            remote(half_send.at[c], half_recv.at[c], h_ss.at[c], h_rs.at[c], partner)
        )
    r_copies = []
    for c in range(CHUNKS):
        cut = slice(c * WIDE, (c + 1) * WIDE)
        own_half[...] = bf(
            dot_cols(back_gate[own_rows, :], gate_w[cut, :])
            + dot_cols(back_up[own_rows, :], up_w[cut, :])
        )
        half_copies[c].wait_recv()
        ret_send[c] = bf(own_half[...].astype(jnp.float32) + half_recv[c].astype(jnp.float32))
        r_copies.append([])
        for n, (dy, dx) in enumerate(PLANE):
            there = rows_at((ring(y, dy) * 4 + ring(x, dx)) * 16, 16)
            r_copies[c].append(
                remote(
                    ret_send.at[c, there],
                    ret_recv.at[c, own_x],
                    r_ss.at[c, n],
                    r_rs.at[c, n],
                    plane_peer(dy, dx),
                )
            )
        ret_recv[c, own_x, :] = ret_send[c, own_x, :]
    sent += half_copies

    stores = []
    for n, (out, grad) in enumerate(((gate_out, back_gate), (up_out, back_up))):
        for c in range(CHUNKS):
            grad_buf[n, c * WIDE : (c + 1) * WIDE, :] = bf(
                dot_rows(rows[c, :, :WIDE], grad[...])
            )
        store = pltpu.make_async_copy(grad_buf.at[n], out.at[0], g_sem.at[n])
        store.start()
        stores.append(store)
    for c in range(CHUNKS):
        down_w[:, c * WIDE : (c + 1) * WIDE] = bf(dot_rows(hidden[...], rows[c, :, WIDE:]))
    store = pltpu.make_async_copy(down_w, down_out.at[0], g_sem.at[2])
    store.start()
    stores.append(store)

    t_copies = []
    for c in range(CHUNKS):
        for copy in r_copies[c]:
            copy.wait_recv()
        tok_send[c] = bf(z_recv[c, :, WIDE:].astype(jnp.float32) + dot(place, ret_recv[c]))
        t_copies.append([])
        for n, dz in enumerate((2, 1, 3)):
            there = rows_at(ring(z, dz) * 32, 32)
            t_copies[c].append(
                remote(
                    tok_send.at[c, there],
                    tok_recv.at[c, own_z],
                    t_ss.at[c, n],
                    t_rs.at[c, n],
                    z_peer(dz),
                )
            )
        tok_recv[c, own_z, :] = tok_send[c, own_z, :]
    a_copies = []
    own_tokens = rows_at(tp * 64, 64)
    for c in range(CHUNKS):
        for copy in t_copies[c]:
            copy.wait_recv()
        token_all[c, own_tokens, :] = bf(dot(z_pick, tok_recv[c]))
        part = token_all.at[c, own_tokens]
        a_copies.append(remote(part, part, a_ss.at[c], a_rs.at[c], partner))
    for c in range(CHUNKS):
        a_copies[c].wait_recv()
        token_ref[:, c * WIDE : (c + 1) * WIDE] = token_all[c]

    sent += note_copies + a_copies
    for group_of in (z_copies, x_copies, r_copies, t_copies):
        for copies in group_of:
            sent += copies
    for copy in sent:
        copy.wait_send()
    for store in stores:
        store.wait()


def expert_layer(experts, weights, mid, cot, gate, up, down):
    b16, f32 = jnp.bfloat16, jnp.float32
    v = pltpu.VMEM
    dma = pltpu.SemaphoreType.DMA
    vmem = pl.BlockSpec(memory_space=pltpu.VMEM)
    hbm = pl.BlockSpec(memory_space=pl.ANY)
    return pl.pallas_call(
        expert_kernel,
        name="expert_layer",
        out_shape=(
            jax.ShapeDtypeStruct((128, 2048), b16),
            jax.ShapeDtypeStruct((1, 2048, 512), b16),
            jax.ShapeDtypeStruct((1, 2048, 512), b16),
            jax.ShapeDtypeStruct((1, 512, 2048), b16),
        ),
        in_specs=[vmem] * 4 + [hbm] * 3,
        out_specs=(vmem, hbm, hbm, hbm),
        scratch_shapes=[
            v((2048, 512), b16),
            v((2048, 512), b16),
            v((512, 2048), b16),
            v((CHUNKS, 128, 2 * WIDE), b16),
            v((128, 128), b16),
            v((CHUNKS, 128, 2 * WIDE), b16),
            v((128, 128), b16),
            v((CHUNKS, 256, 2 * WIDE), b16),
            v((CHUNKS, 512, 2 * WIDE), b16),
            v((512, 512), f32),
            v((512, 512), f32),
            v((512, 512), f32),
            v((512, 512), b16),
            v((512, 512), b16),
            v((512, 512), b16),
            v((CHUNKS, 256, WIDE), b16),
            v((CHUNKS, 256, WIDE), b16),
            v((256, WIDE), b16),
            v((CHUNKS, 256, WIDE), b16),
            v((CHUNKS, 256, WIDE), b16),
            v((CHUNKS, 128, WIDE), b16),
            v((CHUNKS, 128, WIDE), b16),
            v((CHUNKS, 128, WIDE), b16),
            v((2, 2048, 512), b16),
            dma((3,)),
            dma((CHUNKS, 3)),
            dma((CHUNKS, 3)),
            dma((3,)),
            dma((3,)),
            dma((CHUNKS, 15)),
            dma((CHUNKS, 15)),
            dma((CHUNKS, 16)),
            dma((CHUNKS, 16)),
            dma((CHUNKS,)),
            dma((CHUNKS,)),
            dma((CHUNKS, 15)),
            dma((CHUNKS, 15)),
            dma((CHUNKS, 3)),
            dma((CHUNKS, 3)),
            dma((CHUNKS,)),
            dma((CHUNKS,)),
            dma((3,)),
        ],
        compiler_params=pltpu.CompilerParams(
            collective_id=0, has_side_effects=True, vmem_limit_bytes=60 * 1024 * 1024
        ),
        cost_estimate=pl.CostEstimate(
            flops=9_000_000_000, bytes_accessed=14_000_000, transcendentals=300_000
        ),
    )(experts, weights, mid, cot, gate, up, down)


def chain_join(earlier, later):
    return (earlier[0] * later[0], later[0][:, :, None] * earlier[1] + later[1])


def advance(carry_state, inputs):
    factor, addend = inputs
    return (factor[:, :, None] * carry_state + addend, carry_state)


def body(
    mid_rows,
    cotangent,
    route_experts,
    route_weights,
    gate_weight,
    up_weight,
    down_weight,
    out_weight,
    queries,
    key_rows,
    value_rows,
    log_decay,
):
    token_all, *totals = expert_layer(
        route_experts,
        route_weights,
        mid_rows,
        cotangent,
        gate_weight,
        up_weight,
        down_weight,
    )
    local_tokens = queries.shape[0]
    heads_local = queries.shape[1] // DK
    block_count = local_tokens // BLOCK
    query_scaled = queries.astype(jnp.float32).reshape(
        block_count, BLOCK, heads_local, DK
    ) * DK ** (-0.5)
    key_float = key_rows.astype(jnp.float32).reshape(block_count, BLOCK, heads_local, DK)
    value_float = value_rows.astype(jnp.float32).reshape(block_count, BLOCK, heads_local, DV)
    decay_float = log_decay.reshape(block_count, BLOCK, heads_local, DK)
    running_log = jnp.cumsum(decay_float, axis=1)
    block_log = running_log[:, -1]
    query_decayed = query_scaled * jnp.exp(running_log)
    key_inverse = key_float * jnp.exp(-running_log)
    end_factor = jnp.exp(block_log[:, None] - running_log)
    key_to_end = key_float * end_factor
    lower_mask = jnp.tril(jnp.ones((BLOCK, BLOCK), jnp.float32))
    scores = (
        jnp.einsum("nihc,njhc->nhij", query_decayed, key_inverse, precision=precise) * lower_mask
    )
    inner_part = jnp.einsum("nhij,njhv->nihv", scores, value_float, precision=precise)
    increment = jnp.einsum("njhc,njhv->nhcv", key_to_end, value_float, precision=precise)
    block_decay = jnp.exp(block_log)
    zero_state = jnp.zeros((heads_local, DK, DV), jnp.float32)
    local_total, local_prev = lax.scan(advance, zero_state, (block_decay, increment))
    device_decay = jnp.exp(jnp.sum(block_log, axis=0))
    prior_factor = jnp.exp(jnp.cumsum(block_log, axis=0) - block_log)
    identity = (jnp.ones_like(device_decay), jnp.zeros_like(local_total))
    carried = carried_in((device_decay, local_total), SP, chain_join, identity, False)
    incoming = carried[1]
    state_prev = local_prev + prior_factor[:, :, :, None] * incoming[None]
    state_end = device_decay[:, :, None] * incoming + local_total
    raw_out = inner_part + jnp.einsum(
        "nihc,nhcv->nihv", query_decayed, state_prev, precision=precise
    )
    inverse_root = lax.rsqrt(jnp.mean(raw_out * raw_out, axis=-1, keepdims=True) + epsilon)
    normed = raw_out * inverse_root
    normed_rows = normed.astype(jnp.bfloat16).reshape(local_tokens, heads_local * DV)
    out_total = summed_on_arrival(
        lax.dot_general(
            token_all, normed_rows, contract_rows, preferred_element_type=jnp.float32
        ).astype(jnp.bfloat16),
        SP,
        0,
    )
    back_normed = jnp.dot(token_all, out_weight, preferred_element_type=jnp.float32).reshape(
        block_count, BLOCK, heads_local, DV
    )
    back_raw = inverse_root * (
        back_normed - normed * jnp.mean(back_normed * normed, axis=-1, keepdims=True)
    )
    block_back = jnp.einsum("nihc,nihv->nhcv", query_decayed, back_raw, precision=precise)
    device_back = jnp.sum(prior_factor[:, :, :, None] * block_back, axis=0)
    later_part = carried_in((device_decay, device_back), SP, chain_join, identity, True)
    future_state = later_part[1]
    start_state, future_blocks = lax.scan(
        advance, future_state, (block_decay, block_back), reverse=True
    )
    value_dots = (
        jnp.einsum("nihv,njhv->nhij", back_raw, value_float, precision=precise) * lower_mask
    )
    query_part = jnp.einsum("nhij,njhc->nihc", value_dots, key_inverse, precision=precise)
    query_part = query_part + jnp.einsum("nihv,nhcv->nihc", back_raw, state_prev, precision=precise)
    query_back = query_part * jnp.exp(running_log)
    key_back = jnp.exp(-running_log) * jnp.einsum(
        "nhij,nihc->njhc", value_dots, query_decayed, precision=precise
    )
    key_back = key_back + end_factor * jnp.einsum(
        "nhcv,njhv->njhc", future_blocks, value_float, precision=precise
    )
    value_back = jnp.einsum("nhij,nihv->njhv", scores, back_raw, precision=precise)
    value_back = value_back + jnp.einsum(
        "njhc,nhcv->njhv", key_to_end, future_blocks, precision=precise
    )
    running_back = query_scaled * query_back - key_float * key_back
    within_block = jnp.einsum("ji,njhc->nihc", lower_mask, running_back, precision=precise)
    block_sums = jnp.sum(running_back, axis=1)
    strict_upper = jnp.triu(jnp.ones((block_count, block_count), jnp.float32), 1)
    later_blocks = jnp.einsum("nm,mhc->nhc", strict_upper, block_sums, precision=precise)
    cross_term = jnp.sum(state_end * future_state, axis=-1)
    decay_back = within_block + later_blocks[:, None] + cross_term[None, None]
    query_out = (
        (query_back * DK ** (-0.5)).astype(jnp.bfloat16).reshape(local_tokens, heads_local * DK)
    )
    key_out = key_back.astype(jnp.bfloat16).reshape(local_tokens, heads_local * DK)
    value_out = value_back.astype(jnp.bfloat16).reshape(local_tokens, heads_local * DV)
    decay_out = decay_back.reshape(local_tokens, heads_local * DK)
    return (totals[0], totals[1], totals[2], out_total, query_out, key_out, value_out, decay_out)


def solution(mesh):
    split = Mesh(mesh.devices.reshape(4, 4, 4, mesh.shape["tp"]), ("sp_0", "sp_1", "sp_2", "tp"))
    placed = (
        P(SP_TP, None),
        P(SP_TP, None),
        P(SP_TP, None),
        P(SP_TP, None),
        P(SP, None, "tp"),
        P(SP, None, "tp"),
        P(SP, "tp", None),
        P(None, "tp"),
        P(SP, "tp"),
        P(SP, "tp"),
        P(SP, "tp"),
        P(SP, "tp"),
    )
    return jax.shard_map(
        body,
        mesh=split,
        in_specs=placed,
        out_specs=(
            P(SP, None, "tp"),
            P(SP, None, "tp"),
            P(SP, "tp", None),
            P(SP, "tp"),
            P(SP, "tp"),
            P(SP, "tp"),
            P(SP, "tp"),
            P(SP, "tp"),
        ),
        check_vma=False,
    )
```

```python
import jax
import jax.numpy as jnp
from jax import lax
from jax.experimental import pallas as pl
from jax.experimental.pallas import tpu as pltpu
from jax.sharding import Mesh
from jax.sharding import PartitionSpec as P

DK = 128
DV = 256
SP = ("sp_0", "sp_1", "sp_2")
SP_TP = ("sp_0", "sp_1", "sp_2", "tp")
MESH = pl.DeviceIdType.MESH


epsilon = 1e-06
contract_rows = (((0,), (0,)), ((), ()))
contract_cols = (((1,), (1,)), ((), ()))


def silu_parts(pre_gate):
    gate_sigmoid = jax.nn.sigmoid(pre_gate)
    gate_swish = pre_gate * gate_sigmoid
    gate_slope = gate_sigmoid * (1.0 + pre_gate * (1.0 - gate_sigmoid))
    return (gate_swish, gate_slope)


def ring(base, step):
    return lax.rem(base + step, 4)


def rows_at(start, size):
    return pl.ds(pl.multiple_of(start, size), size)


def dot(a, b):
    return lax.dot_general(a, b, (((1,), (0,)), ((), ())), preferred_element_type=jnp.float32)


def dot_rows(a, b):
    return lax.dot_general(a, b, contract_rows, preferred_element_type=jnp.float32)


def dot_cols(a, b):
    return lax.dot_general(a, b, contract_cols, preferred_element_type=jnp.float32)


def ones_where(mask):
    return jnp.where(mask, 1.0, 0.0).astype(jnp.float32)


def bf(a):
    return a.astype(jnp.bfloat16)


def pieces_of(a):
    high = bf(a).astype(jnp.float32)
    mid = bf(a - high).astype(jnp.float32)
    return high, mid, a - high - mid


def split(a):
    high = bf(a)
    return high, bf(a - high.astype(jnp.float32))


def twice(f, a, b):
    high, low = split(a)
    return f(high, b) + f(low, b)


def thrice(f, a, b):
    a_high, a_low = split(a)
    b_high, b_low = split(b)
    return f(a_high, b_high) + (f(a_high, b_low) + f(a_low, b_high))


PLANE = sorted(
    [(dy, dx) for dy in range(4) for dx in range(4) if (dy, dx) != (0, 0)],
    key=lambda o: -(min(o[0], 4 - o[0]) + min(o[1], 4 - o[1])),
)
CHUNKS = 2
WIDE = 2048 // CHUNKS


def layer_kernel(
    experts_ref,
    weights_ref,
    mid_ref,
    cot_ref,
    gate_hbm,
    up_hbm,
    down_hbm,
    out_w_hbm,
    q_ref,
    k_ref,
    v_ref,
    decay_ref,
    gate_out,
    up_out,
    down_out,
    out_out,
    q_out,
    k_out,
    v_out,
    decay_out,
    gate_w,
    up_w,
    down_w,
    z_send,
    z_note_send,
    z_recv,
    z_note,
    x_send,
    rows,
    pre_gate,
    pre_up,
    back_hidden,
    hidden,
    back_gate,
    back_up,
    half_send,
    half_recv,
    own_half,
    ret_send,
    ret_recv,
    tok_send,
    tok_recv,
    token_all,
    grad_buf,
    out_w,
    run_log,
    q_near,
    k_near,
    q_start,
    k_end,
    scores,
    normed,
    root,
    s_local,
    s_send,
    s_recv,
    s_back,
    s_in,
    d_send,
    d_recv,
    n_all,
    b_send,
    b_recv,
    b_back,
    f_in,
    tz,
    o_send,
    o_recv,
    w_sem,
    z_ss,
    z_rs,
    n_ss,
    n_rs,
    x_ss,
    x_rs,
    d_ss,
    d_rs,
    h_ss,
    h_rs,
    r_ss,
    r_rs,
    t_ss,
    t_rs,
    a_ss,
    a_rs,
    g_sem,
    s_ss,
    s_rs,
    e_ss,
    e_rs,
    i_ss,
    i_rs,
    b_ss,
    b_rs,
    f_ss,
    f_rs,
    nz_ss,
    nz_rs,
    tz_ss,
    tz_rs,
    o_ss,
    o_rs,
):
    z, y, x, tp = [lax.axis_index(a) for a in SP_TP]
    other = 1 - tp
    here = y * 4 + x
    mine = tp * 256

    def z_peer(dz):
        return (ring(z, dz), y, x, tp)

    def plane_peer(dy, dx):
        return (z, ring(y, dy), ring(x, dx), tp)

    partner = (z, y, x, other)
    barrier = pltpu.get_barrier_semaphore()
    me = z * 16 + here

    def far_peer(n):
        return (ring(z, n // 16), ring(y, n // 4 % 4), ring(x, n % 4), tp)

    def index_of(peer):
        return peer[0] * 16 + peer[1] * 4 + peer[2]

    def greet(n, carry):
        pl.semaphore_signal(barrier, inc=1, device_id=far_peer(n), device_id_type=MESH)
        return carry

    lax.fori_loop(1, 64, greet, 0)
    pl.semaphore_signal(barrier, inc=1, device_id=partner, device_id_type=MESH)

    loads = []
    for n, (src, dst) in enumerate(((gate_hbm.at[0], gate_w), (up_hbm.at[0], up_w), (down_hbm.at[0], down_w), (out_w_hbm, out_w))):
        load = pltpu.make_async_copy(src, dst, w_sem.at[n])
        load.start()
        loads.append(load)

    def remote(src, dst, ss, rs, peer):
        copy = pltpu.make_async_remote_copy(
            src_ref=src, dst_ref=dst, send_sem=ss, recv_sem=rs, device_id=peer, device_id_type=MESH
        )
        copy.start()
        return copy

    sent = []

    lane = lax.broadcasted_iota(jnp.int32, (64, 128), 1)
    first = experts_ref[:, 0:1]
    second = experts_ref[:, 1:2]
    named_first = ones_where(lane == first)
    named_second = ones_where(lane == second)
    before = bf(
        ones_where(
            lax.broadcasted_iota(jnp.int32, (64, 64), 0)
            > lax.broadcasted_iota(jnp.int32, (64, 64), 1)
        )
    )
    counts = dot(before, bf(named_first + named_second))
    rank_first = jnp.sum(named_first * counts, axis=1, keepdims=True)
    rank_second = jnp.sum(named_second * counts, axis=1, keepdims=True)
    group = lax.shift_right_logical(first, 4)
    in_group = ones_where(lane == group)
    group_rank = jnp.sum(in_group * dot(before, bf(in_group)), axis=1, keepdims=True)
    z_slot = group * 32 + group_rank.astype(jnp.int32)
    z_pick = bf(ones_where(lane == z_slot))
    slot_first = (jnp.bitwise_and(first, 15) * 16).astype(jnp.float32) + rank_first
    slot_second = (jnp.bitwise_and(second, 15) * 16).astype(jnp.float32) + rank_second
    columns = [slot_first, slot_second]
    columns += list(pieces_of(weights_ref[:, 0:1])) + list(pieces_of(weights_ref[:, 1:2]))
    note = ones_where(lane == 8)
    for n, column in enumerate(columns):
        note = jnp.where(lane == n, column, note)
    z_note_send[...] = bf(dot_rows(z_pick, bf(note)))
    for c in range(CHUNKS):
        cut = slice(c * WIDE, (c + 1) * WIDE)
        z_send[c, :, :WIDE] = bf(dot_rows(z_pick, mid_ref[:, cut]))
        z_send[c, :, WIDE:] = bf(dot_rows(z_pick, cot_ref[:, cut]))

    pl.semaphore_wait(barrier, 64)

    z_copies = []
    note_copies = []
    for n, dz in enumerate((2, 1, 3)):
        there = rows_at(ring(z, dz) * 32, 32)
        note_copies.append(
            remote(
                z_note_send.at[there],
                z_note.at[rows_at(z * 32, 32)],
                n_ss.at[n],
                n_rs.at[n],
                z_peer(dz),
            )
        )
    for c in range(CHUNKS):
        z_copies.append([])
        for n, dz in enumerate((2, 1, 3)):
            there = rows_at(ring(z, dz) * 32, 32)
            z_copies[c].append(
                remote(
                    z_send.at[c, there],
                    z_recv.at[c, rows_at(z * 32, 32)],
                    z_ss.at[c, n],
                    z_rs.at[c, n],
                    z_peer(dz),
                )
            )
    own_z = rows_at(z * 32, 32)
    z_note[own_z, :] = z_note_send[own_z, :]
    for c in range(CHUNKS):
        z_recv[c, own_z, :] = z_send[c, own_z, :]

    def all_to_all(make):
        def start(n, carry):
            for copy in make(n):
                copy.start()
            return carry

        lax.fori_loop(1, 64, start, 0)

    def arrived(make):
        def wait(n, carry):
            for copy in make(n):
                copy.wait_recv()
            return carry

        lax.fori_loop(1, 64, wait, 0)

    def drained(make):
        def wait(n, carry):
            for copy in make(n):
                copy.wait_send()
            return carry

        lax.fori_loop(1, 64, wait, 0)

    def flow(src, dst, ss, rs, n, peer):
        return pltpu.make_async_remote_copy(
            src_ref=src,
            dst_ref=dst,
            send_sem=ss.at[n],
            recv_sem=rs.at[n],
            device_id=peer,
            device_id_type=MESH,
        )

    def to_scanner(send, recv, ss, rs, n):
        peer = far_peer(n)
        there = index_of(peer)
        return flow(send.at[rows_at(there * 16, 16)], recv.at[me], ss, rs, n, peer)

    def to_owner(back, incoming, ss, rs, n):
        peer = far_peer(n)
        there = index_of(peer)
        return flow(back.at[there], incoming.at[rows_at(me * 16, 16)], ss, rs, n, peer)

    def decay_flow(n):
        peer = far_peer(n)
        head = index_of(peer) // 16
        return flow(d_send.at[head], d_recv.at[me], e_ss, e_rs, n, peer)

    def state_out(n):
        return (to_scanner(s_send, s_recv, s_ss, s_rs, n), decay_flow(n))

    def state_in(n):
        return (to_owner(s_back, s_in, i_ss, i_rs, n),)

    def grad_out(n):
        return (to_scanner(b_send, b_recv, b_ss, b_rs, n),)

    def grad_in(n):
        return (to_owner(b_back, f_in, f_ss, f_rs, n),)

    def scan(recv, back, reverse):
        def step(n, state):
            at = 63 - n if reverse else n
            back[at] = bf(state)
            return jnp.exp(d_recv[at]) * state + recv[at].astype(jnp.float32)

        lax.fori_loop(0, 64, step, jnp.zeros((16, DK), jnp.float32))

    own_state = rows_at(me * 16, 16)
    square = (128, 128)
    at_row = lax.broadcasted_iota(jnp.int32, square, 0)
    at_col = lax.broadcasted_iota(jnp.int32, square, 1)
    upto = at_row >= at_col
    lower = bf(ones_where(upto))
    upper = bf(ones_where(at_row <= at_col))
    high, mid, low = pieces_of(decay_ref[...])
    run_log[...] = dot(lower, bf(high)) + dot(lower, bf(mid)) + dot(lower, bf(low))
    for h in range(4):
        ks = slice(h * DK, (h + 1) * DK)
        vs = slice(h * DV, (h + 1) * DV)
        running = run_log[:, ks]
        middle = running[63:64]
        total = running[127:128]
        d_send[h] = total
        q_scaled = q_ref[:, ks].astype(jnp.float32) * DK ** (-0.5)
        k_float = k_ref[:, ks].astype(jnp.float32)
        q_near[:, ks] = q_scaled * jnp.exp(running - middle)
        k_near[:, ks] = k_float * jnp.exp(middle - running)
        q_start[:, ks] = q_scaled * jnp.exp(running)
        k_end[:, ks] = k_float * jnp.exp(total - running)
        k_high, k_low = split(k_end[:, ks])
        state = dot_rows(v_ref[:, vs], k_high) + dot_rows(v_ref[:, vs], k_low)
        s_local[vs, :] = state
        s_send[vs, :] = bf(state)
    all_to_all(state_out)
    s_recv[me] = s_send[own_state, :]
    d_recv[me] = d_send[me // 16]

    for copy in note_copies:
        copy.wait_recv()
    got = z_note[...].astype(jnp.float32)
    token_row = lax.broadcasted_iota(jnp.int32, (128, 1), 0)
    offset = lax.shift_right_logical(token_row, 5) * 4
    live = got[:, 8:9] > 0.5
    slot_a = jnp.where(live, got[:, 0:1].astype(jnp.int32) + offset, -1)
    slot_b = jnp.where(live, got[:, 1:2].astype(jnp.int32) + offset, -1)
    slot_lane = lax.broadcasted_iota(jnp.int32, (128, 256), 1)
    place_a = bf(ones_where(slot_lane == slot_a))
    place_b = bf(ones_where(slot_lane == slot_b))
    place = place_a + place_b
    weight_a = got[:, 2:3] + got[:, 3:4] + got[:, 4:5]
    weight_b = got[:, 5:6] + got[:, 6:7] + got[:, 7:8]

    x_copies = []
    own_x = rows_at(here * 16, 16)
    for c in range(CHUNKS):
        for copy in z_copies[c]:
            copy.wait_recv()
        x_send[c, :, :WIDE] = bf(dot_rows(place, z_recv[c, :, :WIDE]))
        cot_part = z_recv[c, :, WIDE:].astype(jnp.float32)
        x_send[c, :, WIDE:] = bf(
            dot_rows(place_a, bf(weight_a * cot_part)) + dot_rows(place_b, bf(weight_b * cot_part))
        )
        x_copies.append([])
        for n, (dy, dx) in enumerate(PLANE):
            there = rows_at((ring(y, dy) * 4 + ring(x, dx)) * 16, 16)
            x_copies[c].append(
                remote(
                    x_send.at[c, there],
                    rows.at[c, rows_at(mine + here * 16, 16)],
                    x_ss.at[c, n],
                    x_rs.at[c, n],
                    plane_peer(dy, dx),
                )
            )
        rows[c, rows_at(mine + here * 16, 16), :] = x_send[c, own_x, :]
        if c == 0:
            arrived(state_out)
            scan(s_recv, s_back, False)
            all_to_all(state_in)
            s_in[own_state, :] = s_back[me]

    for h in range(4):
        ks = slice(h * DK, (h + 1) * DK)
        scores[h] = jnp.where(upto, thrice(dot_cols, q_near[:, ks], k_near[:, ks]), 0.0)
    arrived(state_in)
    for h in range(4):
        ks = slice(h * DK, (h + 1) * DK)
        vs = slice(h * DV, (h + 1) * DV)
        raw = twice(dot, scores[h], v_ref[:, vs]) + twice(dot_cols, q_start[:, ks], s_in[vs, :])
        inverse = lax.rsqrt(jnp.mean(raw * raw, axis=-1, keepdims=True) + epsilon)
        normed[:, vs] = raw * inverse
        root[:, h : h + 1] = inverse
        n_all[rows_at(z * 128, 128), vs] = bf(raw * inverse)
    nz_copies = []
    own_n = n_all.at[rows_at(z * 128, 128)]
    for n, dz in enumerate((2, 1, 3)):
        nz_copies.append(remote(own_n, own_n, nz_ss.at[n], nz_rs.at[n], z_peer(dz)))

    for load in loads:
        load.wait()
    for c in range(CHUNKS):
        shares = []
        for n, (dy, dx) in enumerate(((0, 0),) + tuple(PLANE)):
            if n:
                x_copies[c][n - 1].wait_recv()
            source = ring(y, 4 - dy) * 4 + ring(x, 4 - dx)
            part = rows.at[c, rows_at(mine + source * 16, 16)]
            shares.append(remote(part, part, d_ss.at[c, n], d_rs.at[c, n], partner))
        for copy in shares:
            copy.wait_recv()
        sent += shares
        cut = slice(c * WIDE, (c + 1) * WIDE)
        for ref, weight in ((pre_gate, gate_w), (pre_up, up_w)):
            value = dot(rows[c, :, :WIDE], weight[cut, :])
            ref[...] = value if c == 0 else ref[...] + value
        value = dot_cols(rows[c, :, WIDE:], down_w[:, cut])
        back_hidden[...] = value if c == 0 else back_hidden[...] + value

    gate_swish, gate_slope = silu_parts(pre_gate[...])
    hidden[...] = bf(gate_swish * pre_up[...])
    back_gate[...] = bf(back_hidden[...] * pre_up[...] * gate_slope)
    back_up[...] = bf(back_hidden[...] * gate_swish)

    half_copies = []
    their_rows = rows_at(other * 256, 256)
    own_rows = rows_at(mine, 256)
    for c in range(CHUNKS):
        cut = slice(c * WIDE, (c + 1) * WIDE)
        half_send[c] = bf(
            dot_cols(back_gate[their_rows, :], gate_w[cut, :])
            + dot_cols(back_up[their_rows, :], up_w[cut, :])
        )
        half_copies.append(
            remote(half_send.at[c], half_recv.at[c], h_ss.at[c], h_rs.at[c], partner)
        )
    r_copies = []
    for c in range(CHUNKS):
        cut = slice(c * WIDE, (c + 1) * WIDE)
        own_half[...] = bf(
            dot_cols(back_gate[own_rows, :], gate_w[cut, :])
            + dot_cols(back_up[own_rows, :], up_w[cut, :])
        )
        half_copies[c].wait_recv()
        ret_send[c] = bf(own_half[...].astype(jnp.float32) + half_recv[c].astype(jnp.float32))
        r_copies.append([])
        for n, (dy, dx) in enumerate(PLANE):
            there = rows_at((ring(y, dy) * 4 + ring(x, dx)) * 16, 16)
            r_copies[c].append(
                remote(
                    ret_send.at[c, there],
                    ret_recv.at[c, own_x],
                    r_ss.at[c, n],
                    r_rs.at[c, n],
                    plane_peer(dy, dx),
                )
            )
        ret_recv[c, own_x, :] = ret_send[c, own_x, :]
    sent += half_copies

    stores = []
    for n, (out, grad) in enumerate(((gate_out, back_gate), (up_out, back_up))):
        for c in range(CHUNKS):
            grad_buf[n, c * WIDE : (c + 1) * WIDE, :] = bf(
                dot_rows(rows[c, :, :WIDE], grad[...])
            )
        store = pltpu.make_async_copy(grad_buf.at[n], out.at[0], g_sem.at[n])
        store.start()
        stores.append(store)
    for c in range(CHUNKS):
        down_w[:, c * WIDE : (c + 1) * WIDE] = bf(dot_rows(hidden[...], rows[c, :, WIDE:]))
    store = pltpu.make_async_copy(down_w, down_out.at[0], g_sem.at[2])
    store.start()
    stores.append(store)

    t_copies = []
    for c in range(CHUNKS):
        for copy in r_copies[c]:
            copy.wait_recv()
        tok_send[c] = bf(z_recv[c, :, WIDE:].astype(jnp.float32) + dot(place, ret_recv[c]))
        t_copies.append([])
        for n, dz in enumerate((2, 1, 3)):
            there = rows_at(ring(z, dz) * 32, 32)
            t_copies[c].append(
                remote(
                    tok_send.at[c, there],
                    tok_recv.at[c, own_z],
                    t_ss.at[c, n],
                    t_rs.at[c, n],
                    z_peer(dz),
                )
            )
        tok_recv[c, own_z, :] = tok_send[c, own_z, :]
    a_copies = []
    own_tokens = rows_at(tp * 64, 64)
    each = WIDE // 512
    for c in range(CHUNKS):
        for copy in t_copies[c]:
            copy.wait_recv()
        value = bf(dot(z_pick, tok_recv[c]))
        for j in range(each):
            token_all[c * each + j, own_tokens, :] = value[:, j * 512 : (j + 1) * 512]
        part = token_all.at[c * each : (c + 1) * each, own_tokens]
        a_copies.append(remote(part, part, a_ss.at[c], a_rs.at[c], partner))
    for copy in a_copies:
        copy.wait_recv()
    tz_copies = []
    for n, dz in enumerate((2, 1, 3)):
        tz_copies.append(
            remote(
                token_all.at[ring(z, dz)],
                tz.at[rows_at(z * 128, 128)],
                tz_ss.at[n],
                tz_rs.at[n],
                z_peer(dz),
            )
        )
    tz[rows_at(z * 128, 128), :] = token_all[z]

    back_normed = dot(token_all[0], out_w[0:512, :])
    for j in range(1, 4):
        back_normed = back_normed + dot(token_all[j], out_w[j * 512 : (j + 1) * 512, :])
    back_raw = []
    for h in range(4):
        ks = slice(h * DK, (h + 1) * DK)
        vs = slice(h * DV, (h + 1) * DV)
        back = back_normed[:, vs]
        head_normed = normed[:, vs]
        back = root[:, h : h + 1] * (
            back - head_normed * jnp.mean(back * head_normed, axis=-1, keepdims=True)
        )
        normed[:, vs] = back
        b_send[vs, :] = bf(thrice(dot_rows, back, q_start[:, ks]))
    all_to_all(grad_out)
    b_recv[me] = b_send[own_state, :]

    for copy in tz_copies + nz_copies:
        copy.wait_recv()
    o_copies = []
    o_send[...] = bf(dot_rows(tz[...], n_all[...]))
    for n, (dy, dx) in enumerate(PLANE):
        there = rows_at((ring(y, dy) * 4 + ring(x, dx)) * 32, 32)
        o_copies.append(
            remote(o_send.at[there], o_recv.at[here], o_ss.at[n], o_rs.at[n], plane_peer(dy, dx))
        )
    o_recv[here] = o_send[rows_at(here * 32, 32), :]
    arrived(grad_out)
    scan(b_recv, b_back, True)
    all_to_all(grad_in)
    f_in[own_state, :] = b_back[me]

    for h in range(4):
        ks = slice(h * DK, (h + 1) * DK)
        vs = slice(h * DV, (h + 1) * DV)
        back = normed[:, vs]
        running = run_log[:, ks]
        middle = running[63:64]
        dots = jnp.where(upto, twice(dot_cols, back, v_ref[:, vs]), 0.0)
        q_back = jnp.exp(running - middle) * thrice(dot, dots, k_near[:, ks])
        q_back = q_back + jnp.exp(running) * twice(dot, back, s_in[vs, :])
        k_near[:, ks] = jnp.exp(middle - running) * thrice(dot_rows, dots, q_near[:, ks])
        normed[:, vs] = thrice(dot_rows, scores[h], back)
        q_near[:, ks] = q_back
        q_out[:, ks] = bf(q_back * DK ** (-0.5))
        s_local[vs, :] = jnp.exp(running[127:128]) * s_in[vs, :].astype(jnp.float32) + s_local[vs, :]

    arrived(grad_in)
    for h in range(4):
        ks = slice(h * DK, (h + 1) * DK)
        vs = slice(h * DV, (h + 1) * DV)
        running = run_log[:, ks]
        total = running[127:128]
        future = f_in[vs, :]
        k_back = k_near[:, ks] + jnp.exp(total - running) * dot(v_ref[:, vs], future)
        k_out[:, ks] = bf(k_back)
        v_out[:, vs] = bf(normed[:, vs] + twice(dot_cols, k_end[:, ks], future))
        cross = jnp.sum(s_local[vs, :] * future.astype(jnp.float32), axis=0, keepdims=True)
        q_scaled = q_ref[:, ks].astype(jnp.float32) * DK ** (-0.5)
        change = q_scaled * q_near[:, ks] - k_ref[:, ks].astype(jnp.float32) * k_back
        high, mid, low = pieces_of(change)
        within = dot(upper, bf(high)) + dot(upper, bf(mid)) + dot(upper, bf(low))
        decay_out[:, ks] = within + cross

    for copy in o_copies:
        copy.wait_recv()
    out_total = o_recv[0].astype(jnp.float32)
    for n in range(1, 16):
        out_total = out_total + o_recv[n].astype(jnp.float32)
    out_out[...] = out_total

    sent += nz_copies + tz_copies + o_copies
    for make in (state_out, state_in, grad_out, grad_in):
        drained(make)
    sent += note_copies + a_copies
    for group_of in (z_copies, x_copies, r_copies, t_copies):
        for copies in group_of:
            sent += copies
    for copy in sent:
        copy.wait_send()
    for store in stores:
        store.wait()


def whole_layer(experts, weights, mid, cot, gate, up, down, out_w, queries, keys, values, decay):
    b16, f32 = jnp.bfloat16, jnp.float32
    v = pltpu.VMEM
    dma = pltpu.SemaphoreType.DMA
    vmem = pl.BlockSpec(memory_space=pltpu.VMEM)
    hbm = pl.BlockSpec(memory_space=pl.ANY)
    wide = 2 * WIDE
    pairs = [(CHUNKS, 3), (3,), (CHUNKS, 15), (CHUNKS, 16), (CHUNKS,), (CHUNKS, 15), (CHUNKS, 3), (CHUNKS,)]
    sems = [dma((4,))] + [dma(shape) for shape in pairs for _ in range(2)] + [dma((3,))]
    sems += [dma((64,)) for _ in range(10)]
    sems += [dma(shape) for shape in ((3,), (3,), (15,)) for _ in range(2)]
    return pl.pallas_call(
        layer_kernel,
        name="whole_layer",
        out_shape=(
            jax.ShapeDtypeStruct((1, 2048, 512), b16),
            jax.ShapeDtypeStruct((1, 2048, 512), b16),
            jax.ShapeDtypeStruct((1, 512, 2048), b16),
            jax.ShapeDtypeStruct((32, 1024), f32),
            jax.ShapeDtypeStruct((128, 512), b16),
            jax.ShapeDtypeStruct((128, 512), b16),
            jax.ShapeDtypeStruct((128, 1024), b16),
            jax.ShapeDtypeStruct((128, 512), f32),
        ),
        in_specs=[vmem] * 4 + [hbm] * 4 + [vmem] * 4,
        out_specs=(hbm, hbm, hbm, vmem, vmem, vmem, vmem, vmem),
        scratch_shapes=[
            v((2048, 512), b16),
            v((2048, 512), b16),
            v((512, 2048), b16),
            v((CHUNKS, 128, wide), b16),
            v((128, 128), b16),
            v((CHUNKS, 128, wide), b16),
            v((128, 128), b16),
            v((CHUNKS, 256, wide), b16),
            v((CHUNKS, 512, wide), b16),
            v((512, 512), f32),
            v((512, 512), f32),
            v((512, 512), f32),
            v((512, 512), b16),
            v((512, 512), b16),
            v((512, 512), b16),
            v((CHUNKS, 256, WIDE), b16),
            v((CHUNKS, 256, WIDE), b16),
            v((256, WIDE), b16),
            v((CHUNKS, 256, WIDE), b16),
            v((CHUNKS, 256, WIDE), b16),
            v((CHUNKS, 128, WIDE), b16),
            v((CHUNKS, 128, WIDE), b16),
            v((4, 128, 512), b16),
            v((2, 2048, 512), b16),
            v((2048, 1024), b16),
            v((128, 512), f32),
            v((128, 512), f32),
            v((128, 512), f32),
            v((128, 512), f32),
            v((128, 512), f32),
            v((4, 128, 128), f32),
            v((128, 1024), f32),
            v((128, 128), f32),
            v((1024, 128), f32),
            v((1024, 128), b16),
            v((64, 16, 128), b16),
            v((64, 16, 128), b16),
            v((1024, 128), b16),
            v((4, 1, 128), f32),
            v((64, 1, 128), f32),
            v((512, 1024), b16),
            v((1024, 128), b16),
            v((64, 16, 128), b16),
            v((64, 16, 128), b16),
            v((1024, 128), b16),
            v((512, 512), b16),
            v((512, 1024), b16),
            v((16, 32, 1024), b16),
        ]
        + sems,
        compiler_params=pltpu.CompilerParams(
            collective_id=0, has_side_effects=True, vmem_limit_bytes=63 * 1024 * 1024
        ),
        cost_estimate=pl.CostEstimate(
            flops=11_000_000_000, bytes_accessed=20_000_000, transcendentals=600_000
        ),
    )(experts, weights, mid, cot, gate, up, down, out_w, queries, keys, values, decay)


def body(
    mid_rows,
    cotangent,
    route_experts,
    route_weights,
    gate_weight,
    up_weight,
    down_weight,
    out_weight,
    queries,
    key_rows,
    value_rows,
    log_decay,
):
    return whole_layer(
        route_experts,
        route_weights,
        mid_rows,
        cotangent,
        gate_weight,
        up_weight,
        down_weight,
        out_weight,
        queries,
        key_rows,
        value_rows,
        log_decay,
    )


def solution(mesh):
    split = Mesh(mesh.devices.reshape(4, 4, 4, mesh.shape["tp"]), ("sp_0", "sp_1", "sp_2", "tp"))
    placed = (
        P(SP_TP, None),
        P(SP_TP, None),
        P(SP_TP, None),
        P(SP_TP, None),
        P(SP, None, "tp"),
        P(SP, None, "tp"),
        P(SP, "tp", None),
        P(None, "tp"),
        P(SP, "tp"),
        P(SP, "tp"),
        P(SP, "tp"),
        P(SP, "tp"),
    )
    return jax.shard_map(
        body,
        mesh=split,
        in_specs=placed,
        out_specs=(
            P(SP, None, "tp"),
            P(SP, None, "tp"),
            P(SP, "tp", None),
            P(SP, "tp"),
            P(SP, "tp"),
            P(SP, "tp"),
            P(SP, "tp"),
            P(SP, "tp"),
        ),
        check_vma=False,
    )
```

```python
import jax
import jax.numpy as jnp
from jax import lax
from jax.experimental import pallas as pl
from jax.experimental.pallas import tpu as pltpu
from jax.sharding import Mesh
from jax.sharding import PartitionSpec as P

DK = 128
DV = 256
SP = ("sp_0", "sp_1", "sp_2")
SP_TP = ("sp_0", "sp_1", "sp_2", "tp")
MESH = pl.DeviceIdType.MESH


epsilon = 1e-06
contract_rows = (((0,), (0,)), ((), ()))
contract_cols = (((1,), (1,)), ((), ()))


def silu_parts(pre_gate):
    gate_sigmoid = jax.nn.sigmoid(pre_gate)
    gate_swish = pre_gate * gate_sigmoid
    gate_slope = gate_sigmoid * (1.0 + pre_gate * (1.0 - gate_sigmoid))
    return (gate_swish, gate_slope)


def ring(base, step):
    return lax.rem(base + step, 4)


def rows_at(start, size):
    return pl.ds(pl.multiple_of(start, size), size)


def dot(a, b):
    return lax.dot_general(a, b, (((1,), (0,)), ((), ())), preferred_element_type=jnp.float32)


def dot_rows(a, b):
    return lax.dot_general(a, b, contract_rows, preferred_element_type=jnp.float32)


def dot_cols(a, b):
    return lax.dot_general(a, b, contract_cols, preferred_element_type=jnp.float32)


def ones_where(mask):
    return jnp.where(mask, 1.0, 0.0).astype(jnp.float32)


def bf(a):
    return a.astype(jnp.bfloat16)


def pieces_of(a):
    high = bf(a).astype(jnp.float32)
    mid = bf(a - high).astype(jnp.float32)
    return high, mid, a - high - mid


def split(a):
    high = bf(a)
    return high, bf(a - high.astype(jnp.float32))


def twice(f, a, b):
    high, low = split(a)
    return f(high, b) + f(low, b)


def thrice(f, a, b):
    a_high, a_low = split(a)
    b_high, b_low = split(b)
    return f(a_high, b_high) + (f(a_high, b_low) + f(a_low, b_high))


PLANE = sorted(
    [(dy, dx) for dy in range(4) for dx in range(4) if (dy, dx) != (0, 0)],
    key=lambda o: -(min(o[0], 4 - o[0]) + min(o[1], 4 - o[1])),
)
CHUNKS = 4
WIDE = 2048 // CHUNKS


def layer_kernel(
    experts_ref,
    weights_ref,
    mid_hbm,
    cot_hbm,
    gate_hbm,
    up_hbm,
    down_hbm,
    out_w_hbm,
    q_hbm,
    k_hbm,
    v_hbm,
    decay_hbm,
    gate_out,
    up_out,
    down_out,
    out_out,
    q_out,
    k_out,
    v_out,
    decay_out,
    mid_ref,
    cot_ref,
    gate_w,
    up_w,
    down_w,
    out_w,
    q_ref,
    k_ref,
    v_ref,
    decay_ref,
    z_send,
    z_note_send,
    z_recv,
    z_note,
    x_send,
    rows,
    pre_gate,
    pre_up,
    back_hidden,
    hidden,
    back_gate,
    back_up,
    half_send,
    half_recv,
    ret_send,
    ret_recv,
    tok_send,
    tok_recv,
    token_all,
    run_log,
    q_near,
    k_near,
    q_start,
    k_end,
    scores,
    normed,
    root,
    s_local,
    s_send,
    s_recv,
    s_back,
    s_in,
    d_send,
    d_recv,
    d_factor,
    n_all,
    b_send,
    b_recv,
    b_back,
    f_in,
    tz,
    o_send,
    o_recv,
    w_sem,
    n_sem,
    z_sem,
    x_sem,
    d_sem,
    h_sem,
    r_sem,
    t_sem,
    a_sem,
    s_sem,
    e_sem,
    i_sem,
    b_sem,
    f_sem,
    nz_sem,
    tz_sem,
    o_sem,
):
    z, y, x, tp = [lax.axis_index(a) for a in SP_TP]
    other = 1 - tp
    here = y * 4 + x
    me = z * 16 + here
    mine = tp * 256

    def z_peer(dz):
        return (ring(z, dz), y, x, tp)

    def plane_peer(dy, dx):
        return (z, ring(y, dy), ring(x, dx), tp)

    partner = (z, y, x, other)
    barrier = pltpu.get_barrier_semaphore()
    peers = [z_peer(dz) for dz in (2, 1, 3)] + [plane_peer(*o) for o in PLANE] + [partner]
    for peer in peers:
        pl.semaphore_signal(barrier, inc=1, device_id=peer, device_id_type=MESH)

    loads = []
    moved = (
        (mid_hbm, mid_ref),
        (cot_hbm, cot_ref),
        (decay_hbm, decay_ref),
        (k_hbm, k_ref),
        (v_hbm, v_ref),
        (q_hbm, q_ref),
        (gate_hbm.at[0], gate_w),
        (up_hbm.at[0], up_w),
        (down_hbm.at[0], down_w),
        (out_w_hbm, out_w),
    )
    for n, (src, dst) in enumerate(moved):
        load = pltpu.make_async_copy(src, dst, w_sem.at[n])
        load.start()
        loads.append(load)

    def remote(src, dst, sem, peer):
        copy = pltpu.make_async_remote_copy(
            src_ref=src,
            dst_ref=dst,
            send_sem=sem.at[0],
            recv_sem=sem.at[1],
            device_id=peer,
            device_id_type=MESH,
        )
        copy.start()

    def settle(ref, sem, side):
        pltpu.make_async_copy(ref, ref, sem.at[side]).wait()

    first = experts_ref[0:1, :]
    second = experts_ref[1:2, :]
    expert_row = lax.broadcasted_iota(jnp.int32, (64, 64), 0)
    token_lane = lax.broadcasted_iota(jnp.int32, (64, 64), 1)
    named_first = ones_where(expert_row == first)
    named_second = ones_where(expert_row == second)
    before = bf(ones_where(expert_row < token_lane))
    counts = dot(bf(named_first + named_second), before)
    rank_first = jnp.sum(named_first * counts, axis=0, keepdims=True)
    rank_second = jnp.sum(named_second * counts, axis=0, keepdims=True)
    group = lax.shift_right_logical(first, 4)
    in_group = ones_where(expert_row[:16] == group)
    group_rank = jnp.sum(in_group * dot(bf(in_group), before), axis=0, keepdims=True)
    z_slot = group * 32 + group_rank.astype(jnp.int32)
    slot_row = lax.broadcasted_iota(jnp.int32, (128, 64), 0)
    z_pick = bf(ones_where(slot_row == z_slot))
    slot_first = (jnp.bitwise_and(first, 15) * 16).astype(jnp.float32) + rank_first
    slot_second = (jnp.bitwise_and(second, 15) * 16).astype(jnp.float32) + rank_second
    columns = [slot_first, slot_second]
    columns += list(pieces_of(weights_ref[0:1, :])) + list(pieces_of(weights_ref[1:2, :]))
    note = ones_where(slot_row == 8)
    for n, column in enumerate(columns):
        note = jnp.where(slot_row == n, column, note)
    z_note_send[...] = bf(dot_cols(z_pick, bf(note)))
    own_z = rows_at(z * 32, 32)
    own_x = rows_at(here * 16, 16)

    loads[0].wait()
    loads[1].wait()

    def fill_z(c):
        cut = slice(c * WIDE, (c + 1) * WIDE)
        z_send[c, :, :WIDE] = bf(dot(z_pick, mid_ref[:, cut]))
        z_send[c, :, WIDE:] = bf(dot(z_pick, cot_ref[:, cut]))

    fill_z(0)
    pl.semaphore_wait(barrier, len(peers))

    for dz in (2, 1, 3):
        there = rows_at(ring(z, dz) * 32, 32)
        remote(z_note_send.at[there], z_note.at[own_z], n_sem, z_peer(dz))
    z_note[own_z, :] = z_note_send[own_z, :]
    for c in range(CHUNKS):
        if c:
            fill_z(c)
        for dz in (2, 1, 3):
            there = rows_at(ring(z, dz) * 32, 32)
            remote(z_send.at[c, there], z_recv.at[c, own_z], z_sem.at[c], z_peer(dz))
        z_recv[c, own_z, :] = z_send[c, own_z, :]

    def far(n):
        return (ring(z, n // 16), ring(y, n // 4 % 4), ring(x, n % 4), tp)

    def all_to_all(send):
        def start(n, carry):
            peer = far(n)
            send(peer, peer[0] * 16 + peer[1] * 4 + peer[2])
            return carry

        lax.fori_loop(1, 64, start, 0)

    def state_out(peer, there):
        remote(s_send.at[rows_at(there * 16, 16)], s_recv.at[me], s_sem, peer)
        remote(d_send.at[there // 16], d_recv.at[me], e_sem, peer)

    def state_in(peer, there):
        remote(s_back.at[there], s_in.at[own_state], i_sem, peer)

    def grad_out(peer, there):
        remote(b_send.at[rows_at(there * 16, 16)], b_recv.at[me], b_sem, peer)

    def grad_in(peer, there):
        remote(b_back.at[there], f_in.at[own_state], f_sem, peer)

    def scan(recv, back, reverse):
        state = jnp.zeros((16, DK), jnp.float32)
        for n in range(64):
            at = 63 - n if reverse else n
            back[at] = bf(state)
            state = d_factor[at] * state + recv[at].astype(jnp.float32)

    own_state = rows_at(me * 16, 16)
    square = (128, 128)
    at_row = lax.broadcasted_iota(jnp.int32, square, 0)
    at_col = lax.broadcasted_iota(jnp.int32, square, 1)
    upto = at_row >= at_col
    lower = bf(ones_where(upto))
    upper = bf(ones_where(at_row <= at_col))
    for load in loads[2:6]:
        load.wait()
    high, mid, low = pieces_of(decay_ref[...])
    run_log[...] = dot(lower, bf(high)) + dot(lower, bf(mid)) + dot(lower, bf(low))
    for h in range(4):
        ks = slice(h * DK, (h + 1) * DK)
        vs = slice(h * DV, (h + 1) * DV)
        running = run_log[:, ks]
        total = running[127:128]
        d_send[h] = total
        k_end[:, ks] = k_ref[:, ks].astype(jnp.float32) * jnp.exp(total - running)
        k_high, k_low = split(k_end[:, ks])
        state = dot_rows(v_ref[:, vs], k_high) + dot_rows(v_ref[:, vs], k_low)
        s_local[vs, :] = state
        s_send[vs, :] = bf(state)

    settle(z_note.at[0:96], n_sem, 1)
    all_to_all(state_out)
    s_recv[me] = s_send[own_state, :]
    d_recv[me] = d_send[me // 16]
    got = z_note[...].astype(jnp.float32)
    token_row = lax.broadcasted_iota(jnp.int32, (128, 1), 0)
    offset = lax.shift_right_logical(token_row, 5) * 4
    live = got[:, 8:9] > 0.5
    slot_a = jnp.where(live, got[:, 0:1].astype(jnp.int32) + offset, -1)
    slot_b = jnp.where(live, got[:, 1:2].astype(jnp.int32) + offset, -1)
    slot_lane = lax.broadcasted_iota(jnp.int32, (128, 256), 1)
    place_a = bf(ones_where(slot_lane == slot_a))
    place_b = bf(ones_where(slot_lane == slot_b))
    place = place_a + place_b
    weight_a = got[:, 2:3] + got[:, 3:4] + got[:, 4:5]
    weight_b = got[:, 5:6] + got[:, 6:7] + got[:, 7:8]

    for c in range(CHUNKS):
        settle(z_recv.at[c, 0:96], z_sem.at[c], 1)
        x_send[c, :, :WIDE] = bf(dot_rows(place, z_recv[c, :, :WIDE]))
        cot_part = z_recv[c, :, WIDE:].astype(jnp.float32)
        x_send[c, :, WIDE:] = bf(
            dot_rows(place_a, bf(weight_a * cot_part)) + dot_rows(place_b, bf(weight_b * cot_part))
        )
        for dy, dx in PLANE:
            there = rows_at((ring(y, dy) * 4 + ring(x, dx)) * 16, 16)
            remote(
                x_send.at[c, there],
                rows.at[c, rows_at(mine + here * 16, 16)],
                x_sem.at[c],
                plane_peer(dy, dx),
            )
        rows[c, rows_at(mine + here * 16, 16), :] = x_send[c, own_x, :]
        if c == 1:
            settle(s_recv.at[0:63], s_sem, 1)
            settle(d_recv.at[0:63], e_sem, 1)
            d_factor[...] = jnp.exp(d_recv[...])
            scan(s_recv, s_back, False)
            all_to_all(state_in)
            s_in[own_state, :] = s_back[me]

    for h in range(4):
        ks = slice(h * DK, (h + 1) * DK)
        running = run_log[:, ks]
        middle = running[63:64]
        q_scaled = q_ref[:, ks].astype(jnp.float32) * DK ** (-0.5)
        q_near[:, ks] = q_scaled * jnp.exp(running - middle)
        k_near[:, ks] = k_ref[:, ks].astype(jnp.float32) * jnp.exp(middle - running)
        q_start[:, ks] = q_scaled * jnp.exp(running)
        scores[h] = jnp.where(upto, thrice(dot_cols, q_near[:, ks], k_near[:, ks]), 0.0)
    settle(s_in.at[0:1008], i_sem, 1)
    for h in range(4):
        ks = slice(h * DK, (h + 1) * DK)
        vs = slice(h * DV, (h + 1) * DV)
        raw = twice(dot, scores[h], v_ref[:, vs]) + twice(dot_cols, q_start[:, ks], s_in[vs, :])
        inverse = lax.rsqrt(jnp.mean(raw * raw, axis=-1, keepdims=True) + epsilon)
        normed[:, vs] = raw * inverse
        root[:, h : h + 1] = inverse
        n_all[rows_at(z * 128, 128), vs] = bf(raw * inverse)
    own_n = n_all.at[rows_at(z * 128, 128)]
    for dz in (2, 1, 3):
        remote(own_n, own_n, nz_sem, z_peer(dz))

    for load in loads[6:]:
        load.wait()
    their_rows = rows_at(other * 256, 256)
    own_rows = rows_at(mine, 256)

    def gather_up(c, part):
        cut = slice(c * WIDE, (c + 1) * WIDE)
        for ref, value in (
            (pre_gate, dot(rows[c, part, :WIDE], gate_w[cut, :])),
            (pre_up, dot(rows[c, part, :WIDE], up_w[cut, :])),
            (back_hidden, dot_cols(rows[c, part, WIDE:], down_w[:, cut])),
        ):
            ref[part, :] = value if c == 0 else ref[part, :] + value

    for c in range(CHUNKS):
        settle(rows.at[c, 0:240], x_sem.at[c], 1)
        remote(rows.at[c, own_rows], rows.at[c, own_rows], d_sem.at[c], partner)
        gather_up(c, own_rows)
        settle(rows.at[c, 0:256], d_sem.at[c], 1)
        gather_up(c, their_rows)

    gate_swish, gate_slope = silu_parts(pre_gate[...])
    hidden[...] = bf(gate_swish * pre_up[...])
    back_gate[...] = bf(back_hidden[...] * pre_up[...] * gate_slope)
    back_up[...] = bf(back_hidden[...] * gate_swish)

    def half_of(part, c):
        cut = slice(c * WIDE, (c + 1) * WIDE)
        return bf(
            dot_cols(back_gate[part, :], gate_w[cut, :]) + dot_cols(back_up[part, :], up_w[cut, :])
        )

    def send_half(c):
        half_send[c] = half_of(their_rows, c)
        remote(half_send.at[c], half_recv.at[c], h_sem.at[c], partner)

    def give_back(c):
        own_half = half_of(own_rows, c).astype(jnp.float32)
        settle(half_recv.at[c], h_sem.at[c], 1)
        ret_send[c] = bf(own_half + half_recv[c].astype(jnp.float32))
        for dy, dx in PLANE:
            there = rows_at((ring(y, dy) * 4 + ring(x, dx)) * 16, 16)
            remote(ret_send.at[c, there], ret_recv.at[c, own_x], r_sem.at[c], plane_peer(dy, dx))
        ret_recv[c, own_x, :] = ret_send[c, own_x, :]

    send_half(0)
    for c in range(CHUNKS):
        if c + 1 < CHUNKS:
            send_half(c + 1)
        give_back(c)

    for c in range(CHUNKS):
        cut = slice(c * WIDE, (c + 1) * WIDE)
        gate_out[0, cut, :] = bf(dot_rows(rows[c, :, :WIDE], back_gate[...]))
        up_out[0, cut, :] = bf(dot_rows(rows[c, :, :WIDE], back_up[...]))
        down_out[0, :, cut] = bf(dot_rows(hidden[...], rows[c, :, WIDE:]))

    own_tokens = rows_at(tp * 64, 64)

    def to_tokens(c):
        settle(ret_recv.at[c, 0:240], r_sem.at[c], 1)
        tok_send[c] = bf(z_recv[c, :, WIDE:].astype(jnp.float32) + dot(place, ret_recv[c]))
        for dz in (2, 1, 3):
            there = rows_at(ring(z, dz) * 32, 32)
            remote(tok_send.at[c, there], tok_recv.at[c, own_z], t_sem.at[c], z_peer(dz))
        tok_recv[c, own_z, :] = tok_send[c, own_z, :]

    def share_tokens(c):
        settle(tok_recv.at[c, 0:96], t_sem.at[c], 1)
        token_all[c, own_tokens, :] = bf(dot_rows(z_pick, tok_recv[c]))
        part = token_all.at[c, own_tokens]
        remote(part, part, a_sem.at[c], partner)

    def use_tokens(c, total):
        settle(token_all.at[c, 0:64], a_sem.at[c], 1)

        @pl.when(z != c)
        def send():
            remote(token_all.at[c], tz.at[rows_at(z * 128, 128)], tz_sem, (c, y, x, tp))

        value = dot(token_all[c], out_w[c * WIDE : (c + 1) * WIDE, :])
        return value if total is None else total + value

    to_tokens(0)
    to_tokens(1)
    share_tokens(0)
    to_tokens(2)
    share_tokens(1)
    back_normed = use_tokens(0, None)
    to_tokens(3)
    share_tokens(2)
    back_normed = use_tokens(1, back_normed)
    share_tokens(3)
    back_normed = use_tokens(2, back_normed)
    back_normed = use_tokens(3, back_normed)

    for h in range(4):
        ks = slice(h * DK, (h + 1) * DK)
        vs = slice(h * DV, (h + 1) * DV)
        back = back_normed[:, vs]
        head_normed = normed[:, vs]
        back = root[:, h : h + 1] * (
            back - head_normed * jnp.mean(back * head_normed, axis=-1, keepdims=True)
        )
        normed[:, vs] = back
        b_send[vs, :] = bf(thrice(dot_rows, back, q_start[:, ks]))
    all_to_all(grad_out)
    b_recv[me] = b_send[own_state, :]

    tz[rows_at(z * 128, 128), :] = token_all[z]
    settle(tz.at[0:384], tz_sem, 1)
    settle(n_all.at[0:384], nz_sem, 1)
    o_send[...] = bf(dot_rows(tz[...], n_all[...]))

    def spread(offsets):
        for dy, dx in offsets:
            there = rows_at((ring(y, dy) * 4 + ring(x, dx)) * 32, 32)
            remote(o_send.at[there], o_recv.at[here], o_sem, plane_peer(dy, dx))

    spread(PLANE[:7])
    o_recv[here] = o_send[rows_at(here * 32, 32), :]
    settle(b_recv.at[0:63], b_sem, 1)
    scan(b_recv, b_back, True)
    all_to_all(grad_in)
    f_in[own_state, :] = b_back[me]
    spread(PLANE[7:])

    for h in range(4):
        ks = slice(h * DK, (h + 1) * DK)
        vs = slice(h * DV, (h + 1) * DV)
        back = normed[:, vs]
        running = run_log[:, ks]
        middle = running[63:64]
        dots = jnp.where(upto, twice(dot_cols, back, v_ref[:, vs]), 0.0)
        q_back = jnp.exp(running - middle) * thrice(dot, dots, k_near[:, ks])
        q_back = q_back + jnp.exp(running) * twice(dot, back, s_in[vs, :])
        k_near[:, ks] = jnp.exp(middle - running) * thrice(dot_rows, dots, q_near[:, ks])
        normed[:, vs] = thrice(dot_rows, scores[h], back)
        q_near[:, ks] = q_back
        q_out[:, ks] = bf(q_back * DK ** (-0.5))
        s_local[vs, :] = jnp.exp(running[127:128]) * s_in[vs, :].astype(jnp.float32) + s_local[vs, :]

    settle(z_note_send.at[0:96], n_sem, 0)
    settle(s_send.at[0:1008], s_sem, 0)
    settle(d_recv.at[0:63], e_sem, 0)
    settle(s_back.at[0:63], i_sem, 0)
    settle(n_all.at[0:384], nz_sem, 0)
    settle(tz.at[0:384], tz_sem, 0)
    settle(b_send.at[0:1008], b_sem, 0)
    for c in range(CHUNKS):
        settle(z_send.at[c, 0:96], z_sem.at[c], 0)
        settle(x_send.at[c, 0:240], x_sem.at[c], 0)
        settle(rows.at[c, 0:256], d_sem.at[c], 0)
        settle(half_send.at[c], h_sem.at[c], 0)
        settle(ret_send.at[c, 0:240], r_sem.at[c], 0)
        settle(tok_send.at[c, 0:96], t_sem.at[c], 0)
        settle(token_all.at[c, 0:64], a_sem.at[c], 0)
    settle(f_in.at[0:1008], f_sem, 1)
    for h in range(4):
        ks = slice(h * DK, (h + 1) * DK)
        vs = slice(h * DV, (h + 1) * DV)
        running = run_log[:, ks]
        total = running[127:128]
        future = f_in[vs, :]
        k_back = k_near[:, ks] + jnp.exp(total - running) * dot(v_ref[:, vs], future)
        k_out[:, ks] = bf(k_back)
        v_out[:, vs] = bf(normed[:, vs] + twice(dot_cols, k_end[:, ks], future))
        cross = jnp.sum(s_local[vs, :] * future.astype(jnp.float32), axis=0, keepdims=True)
        q_scaled = q_ref[:, ks].astype(jnp.float32) * DK ** (-0.5)
        change = q_scaled * q_near[:, ks] - k_ref[:, ks].astype(jnp.float32) * k_back
        high, mid, low = pieces_of(change)
        within = dot(upper, bf(high)) + dot(upper, bf(mid)) + dot(upper, bf(low))
        decay_out[:, ks] = within + cross

    settle(o_recv.at[0:15], o_sem, 1)
    out_total = o_recv[0].astype(jnp.float32)
    for n in range(1, 16):
        out_total = out_total + o_recv[n].astype(jnp.float32)
    out_out[...] = out_total
    settle(o_recv.at[0:15], o_sem, 0)
    settle(b_back.at[0:63], f_sem, 0)


def finish_kernel(*refs):
    count = len(refs) // 2
    sems = refs[-1]
    copies = []
    for n in range(count):
        copy = pltpu.make_async_copy(refs[n], refs[count + n], sems.at[n])
        copy.start()
        copies.append(copy)
    for copy in copies:
        copy.wait()


def whole_layer(experts, weights, mid, cot, gate, up, down, out_w, queries, keys, values, decay):
    b16, f32 = jnp.bfloat16, jnp.float32
    v = pltpu.VMEM
    dma = pltpu.SemaphoreType.DMA
    vmem = pl.BlockSpec(memory_space=pltpu.VMEM)
    hbm = pl.BlockSpec(memory_space=pl.ANY)
    outs = (
        ((1, 2048, 512), b16),
        ((1, 2048, 512), b16),
        ((1, 512, 2048), b16),
        ((32, 1024), f32),
        ((128, 512), b16),
        ((128, 512), b16),
        ((128, 1024), b16),
        ((128, 512), f32),
    )
    scratch = (
        ((64, 2048), b16),
        ((64, 2048), b16),
        ((2048, 512), b16),
        ((2048, 512), b16),
        ((512, 2048), b16),
        ((2048, 1024), b16),
        ((128, 512), b16),
        ((128, 512), b16),
        ((128, 1024), b16),
        ((128, 512), f32),
        ((CHUNKS, 128, 2 * WIDE), b16),
        ((128, 128), b16),
        ((CHUNKS, 128, 2 * WIDE), b16),
        ((128, 128), b16),
        ((CHUNKS, 256, 2 * WIDE), b16),
        ((CHUNKS, 512, 2 * WIDE), b16),
        ((512, 512), f32),
        ((512, 512), f32),
        ((512, 512), f32),
        ((512, 512), b16),
        ((512, 512), b16),
        ((512, 512), b16),
        ((CHUNKS, 256, WIDE), b16),
        ((CHUNKS, 256, WIDE), b16),
        ((CHUNKS, 256, WIDE), b16),
        ((CHUNKS, 256, WIDE), b16),
        ((CHUNKS, 128, WIDE), b16),
        ((CHUNKS, 128, WIDE), b16),
        ((4, 128, 512), b16),
        ((128, 512), f32),
        ((128, 512), f32),
        ((128, 512), f32),
        ((128, 512), f32),
        ((128, 512), f32),
        ((4, 128, 128), f32),
        ((128, 1024), f32),
        ((128, 128), f32),
        ((1024, 128), f32),
        ((1024, 128), b16),
        ((64, 16, 128), b16),
        ((64, 16, 128), b16),
        ((1024, 128), b16),
        ((4, 1, 128), f32),
        ((64, 1, 128), f32),
        ((64, 1, 128), f32),
        ((512, 1024), b16),
        ((1024, 128), b16),
        ((64, 16, 128), b16),
        ((64, 16, 128), b16),
        ((1024, 128), b16),
        ((512, 512), b16),
        ((512, 1024), b16),
        ((16, 32, 1024), b16),
    )
    two, many = (2,), (CHUNKS, 2)
    sems = [(10,), two] + [many] * 7 + [two] * 8
    made = pl.pallas_call(
        layer_kernel,
        name="whole_layer",
        out_shape=tuple(v(shape, kind) for shape, kind in outs),
        in_specs=[vmem] * 2 + [hbm] * 10,
        out_specs=(vmem,) * 8,
        scratch_shapes=[v(shape, kind) for shape, kind in scratch] + [dma(shape) for shape in sems],
        compiler_params=pltpu.CompilerParams(
            collective_id=0, has_side_effects=True, vmem_limit_bytes=50 * 1024 * 1024
        ),
        cost_estimate=pl.CostEstimate(
            flops=11_000_000_000, bytes_accessed=20_000_000, transcendentals=600_000
        ),
    )(experts.T, weights.T, mid, cot, gate, up, down, out_w, queries, keys, values, decay)
    return pl.pallas_call(
        finish_kernel,
        name="finish",
        out_shape=tuple(jax.ShapeDtypeStruct(shape, kind) for shape, kind in outs),
        in_specs=[vmem] * 8,
        out_specs=(hbm,) * 8,
        scratch_shapes=[dma((8,))],
        compiler_params=pltpu.CompilerParams(vmem_limit_bytes=1024 * 1024),
    )(*[pltpu.with_memory_space_constraint(a, pltpu.VMEM) for a in made])


def body(
    mid_rows,
    cotangent,
    route_experts,
    route_weights,
    gate_weight,
    up_weight,
    down_weight,
    out_weight,
    queries,
    key_rows,
    value_rows,
    log_decay,
):
    return whole_layer(
        route_experts,
        route_weights,
        mid_rows,
        cotangent,
        gate_weight,
        up_weight,
        down_weight,
        out_weight,
        queries,
        key_rows,
        value_rows,
        log_decay,
    )


def solution(mesh):
    split = Mesh(mesh.devices.reshape(4, 4, 4, mesh.shape["tp"]), ("sp_0", "sp_1", "sp_2", "tp"))
    placed = (
        P(SP_TP, None),
        P(SP_TP, None),
        P(SP_TP, None),
        P(SP_TP, None),
        P(SP, None, "tp"),
        P(SP, None, "tp"),
        P(SP, "tp", None),
        P(None, "tp"),
        P(SP, "tp"),
        P(SP, "tp"),
        P(SP, "tp"),
        P(SP, "tp"),
    )
    return jax.shard_map(
        body,
        mesh=split,
        in_specs=placed,
        out_specs=(
            P(SP, None, "tp"),
            P(SP, None, "tp"),
            P(SP, "tp", None),
            P(SP, "tp"),
            P(SP, "tp"),
            P(SP, "tp"),
            P(SP, "tp"),
            P(SP, "tp"),
        ),
        check_vma=False,
    )
```

```python
import jax
import jax.numpy as jnp
from jax import lax
from jax.experimental import pallas as pl
from jax.experimental.pallas import tpu as pltpu
from jax.sharding import Mesh
from jax.sharding import PartitionSpec as P

DK = 128
DV = 256
SP = ("sp_0", "sp_1", "sp_2")
SP_TP = ("sp_0", "sp_1", "sp_2", "tp")
MESH = pl.DeviceIdType.MESH


epsilon = 1e-06
contract_rows = (((0,), (0,)), ((), ()))
contract_cols = (((1,), (1,)), ((), ()))


def silu_parts(pre_gate):
    gate_sigmoid = jax.nn.sigmoid(pre_gate)
    gate_swish = pre_gate * gate_sigmoid
    gate_slope = gate_sigmoid * (1.0 + pre_gate * (1.0 - gate_sigmoid))
    return (gate_swish, gate_slope)


def ring(base, step):
    return lax.rem(base + step, 4)


def rows_at(start, size):
    return pl.ds(pl.multiple_of(start, size), size)


def dot(a, b):
    return lax.dot_general(a, b, (((1,), (0,)), ((), ())), preferred_element_type=jnp.float32)


def dot_rows(a, b):
    return lax.dot_general(a, b, contract_rows, preferred_element_type=jnp.float32)


def dot_cols(a, b):
    return lax.dot_general(a, b, contract_cols, preferred_element_type=jnp.float32)


def ones_where(mask):
    return jnp.where(mask, 1.0, 0.0).astype(jnp.float32)


def bf(a):
    return a.astype(jnp.bfloat16)


def total_of(parts):
    total = parts[0].astype(jnp.float32) + parts[1].astype(jnp.float32)
    return total + parts[2].astype(jnp.float32) + parts[3].astype(jnp.float32)


def pieces_of(a):
    high = bf(a).astype(jnp.float32)
    mid = bf(a - high).astype(jnp.float32)
    return high, mid, a - high - mid


def split(a):
    high = bf(a)
    return high, bf(a - high.astype(jnp.float32))


def twice(f, a, b):
    high, low = split(a)
    return f(high, b) + f(low, b)


def thrice(f, a, b):
    a_high, a_low = split(a)
    b_high, b_low = split(b)
    return f(a_high, b_high) + (f(a_high, b_low) + f(a_low, b_high))


PLANE = sorted(
    [(dy, dx) for dy in range(4) for dx in range(4) if (dy, dx) != (0, 0)],
    key=lambda o: -(min(o[0], 4 - o[0]) + min(o[1], 4 - o[1])),
)
FAR = sorted(
    [(i, j, k) for i in range(4) for j in range(4) for k in range(4) if i + j + k],
    key=lambda o: -sum(min(d, 4 - d) for d in o),
)
CHUNKS = 4
WIDE = 2048 // CHUNKS


def layer_kernel(
    experts_ref,
    weights_ref,
    mid_hbm,
    cot_hbm,
    gate_hbm,
    up_hbm,
    down_hbm,
    out_w_hbm,
    q_hbm,
    k_hbm,
    v_hbm,
    decay_hbm,
    gate_out,
    up_out,
    down_out,
    out_out,
    q_out,
    k_out,
    v_out,
    decay_out,
    mid_ref,
    cot_ref,
    gate_w,
    up_w,
    down_w,
    out_w,
    q_ref,
    k_ref,
    v_ref,
    decay_ref,
    z_send,
    z_note_send,
    z_recv,
    z_note,
    x_send,
    rows,
    pre_gate,
    pre_up,
    back_hidden,
    hidden,
    back_gate,
    back_up,
    half_send,
    half_recv,
    ret_send,
    ret_recv,
    tok_send,
    tok_recv,
    token_all,
    run_log,
    q_near,
    k_near,
    q_start,
    k_end,
    scores,
    normed,
    root,
    s_local,
    s_send,
    s_recv,
    s_back,
    s_in,
    d_send,
    d_recv,
    d_factor,
    n_all,
    b_send,
    b_recv,
    b_back,
    f_in,
    tz,
    o_send,
    o_recv,
    o_part,
    o_last,
    p_send,
    p_recv,
    p_part,
    p_last,
    w_sem,
    n_sem,
    z_sem,
    x_sem,
    d_sem,
    h_sem,
    r_sem,
    t_sem,
    a_sem,
    s_sem,
    e_sem,
    i_sem,
    b_sem,
    f_sem,
    nz_sem,
    tz_sem,
    tz2_sem,
    o_sem,
    o2_sem,
    p_sem,
    p2_sem,
):
    z, y, x, tp = [lax.axis_index(a) for a in SP_TP]
    other = 1 - tp
    here = y * 4 + x
    me = z * 16 + here
    mine = tp * 256

    def z_peer(dz):
        return (ring(z, dz), y, x, tp)

    def plane_peer(dy, dx):
        return (z, ring(y, dy), ring(x, dx), tp)

    partner = (z, y, x, other)
    barrier = pltpu.get_barrier_semaphore()
    peers = [z_peer(dz) for dz in (2, 1, 3)] + [plane_peer(*o) for o in PLANE] + [partner]
    for peer in peers:
        pl.semaphore_signal(barrier, inc=1, device_id=peer, device_id_type=MESH)

    loads = []
    moved = (
        (mid_hbm, mid_ref),
        (cot_hbm, cot_ref),
        (decay_hbm, decay_ref),
        (k_hbm, k_ref),
        (v_hbm, v_ref),
        (q_hbm, q_ref),
        (gate_hbm.at[0], gate_w),
        (up_hbm.at[0], up_w),
        (down_hbm.at[0], down_w),
        (out_w_hbm, out_w),
    )
    for n, (src, dst) in enumerate(moved):
        load = pltpu.make_async_copy(src, dst, w_sem.at[n])
        load.start()
        loads.append(load)

    def remote(src, dst, sem, peer):
        copy = pltpu.make_async_remote_copy(
            src_ref=src,
            dst_ref=dst,
            send_sem=sem.at[0],
            recv_sem=sem.at[1],
            device_id=peer,
            device_id_type=MESH,
        )
        copy.start()

    def settle(ref, sem, side):
        pltpu.make_async_copy(ref, ref, sem.at[side]).wait()

    first = experts_ref[0:1, :]
    second = experts_ref[1:2, :]
    expert_row = lax.broadcasted_iota(jnp.int32, (64, 64), 0)
    token_lane = lax.broadcasted_iota(jnp.int32, (64, 64), 1)
    named_first = ones_where(expert_row == first)
    named_second = ones_where(expert_row == second)
    before = bf(ones_where(expert_row < token_lane))
    counts = dot(bf(named_first + named_second), before)
    rank_first = jnp.sum(named_first * counts, axis=0, keepdims=True)
    rank_second = jnp.sum(named_second * counts, axis=0, keepdims=True)
    group = lax.shift_right_logical(first, 4)
    in_group = ones_where(expert_row[:16] == group)
    group_rank = jnp.sum(in_group * dot(bf(in_group), before), axis=0, keepdims=True)
    z_slot = group * 32 + group_rank.astype(jnp.int32)
    slot_row = lax.broadcasted_iota(jnp.int32, (128, 64), 0)
    z_pick = bf(ones_where(slot_row == z_slot))
    slot_first = (jnp.bitwise_and(first, 15) * 16).astype(jnp.float32) + rank_first
    slot_second = (jnp.bitwise_and(second, 15) * 16).astype(jnp.float32) + rank_second
    columns = [slot_first, slot_second]
    columns += list(pieces_of(weights_ref[0:1, :])) + list(pieces_of(weights_ref[1:2, :]))
    note = ones_where(slot_row == 8)
    for n, column in enumerate(columns):
        note = jnp.where(slot_row == n, column, note)
    z_note_send[...] = bf(dot_cols(z_pick, bf(note)))
    own_z = rows_at(z * 32, 32)
    own_x = rows_at(here * 16, 16)

    loads[0].wait()
    loads[1].wait()

    def fill_z(c):
        cut = slice(c * WIDE, (c + 1) * WIDE)
        z_send[c, :, :WIDE] = bf(dot(z_pick, mid_ref[:, cut]))
        z_send[c, :, WIDE:] = bf(dot(z_pick, cot_ref[:, cut]))

    fill_z(0)
    pl.semaphore_wait(barrier, len(peers))

    for dz in (2, 1, 3):
        there = rows_at(ring(z, dz) * 32, 32)
        remote(z_note_send.at[there], z_note.at[own_z], n_sem, z_peer(dz))
    z_note[own_z, :] = z_note_send[own_z, :]

    def send_z(c):
        for dz in (2, 1, 3):
            there = rows_at(ring(z, dz) * 32, 32)
            remote(z_send.at[c, there], z_recv.at[c, own_z], z_sem.at[c], z_peer(dz))
        z_recv[c, own_z, :] = z_send[c, own_z, :]

    send_z(0)

    along_z, along_y, along_x = [[ring(a, d) for d in range(4)] for a in (z, y, x)]
    bases = [[along_z[i] * 16 + along_y[j] * 4 for j in range(4)] for i in range(4)]

    def all_to_all(send):
        for i, j, k in FAR:
            peer = (along_z[i], along_y[j], along_x[k], tp)
            send(peer, bases[i][j] + along_x[k])

    def state_out(peer, there):
        remote(s_send.at[rows_at(there * 16, 16)], s_recv.at[me], s_sem, peer)
        remote(d_send.at[there // 16], d_recv.at[me], e_sem, peer)

    def state_in(peer, there):
        remote(s_back.at[there], s_in.at[own_state], i_sem, peer)

    def grad_out(peer, there):
        remote(b_send.at[rows_at(there * 16, 16)], b_recv.at[me], b_sem, peer)

    def grad_in(peer, there):
        remote(b_back.at[there], f_in.at[own_state], f_sem, peer)

    def scan(recv, back, reverse):
        state = jnp.zeros((16, DK), jnp.float32)
        for n in range(64):
            at = 63 - n if reverse else n
            back[at] = bf(state)
            state = d_factor[at] * state + recv[at].astype(jnp.float32)

    own_state = rows_at(me * 16, 16)
    square = (128, 128)
    at_row = lax.broadcasted_iota(jnp.int32, square, 0)
    at_col = lax.broadcasted_iota(jnp.int32, square, 1)
    upto = at_row >= at_col
    lower = bf(ones_where(upto))
    upper = bf(ones_where(at_row <= at_col))
    for load in loads[2:6]:
        load.wait()
    high, mid, low = pieces_of(decay_ref[...])
    run_log[...] = dot(lower, bf(high)) + dot(lower, bf(mid)) + dot(lower, bf(low))
    for h in range(4):
        ks = slice(h * DK, (h + 1) * DK)
        vs = slice(h * DV, (h + 1) * DV)
        running = run_log[:, ks]
        total = running[127:128]
        d_send[h] = total
        k_end[:, ks] = k_ref[:, ks].astype(jnp.float32) * jnp.exp(total - running)
        k_high, k_low = split(k_end[:, ks])
        state = dot_rows(v_ref[:, vs], k_high) + dot_rows(v_ref[:, vs], k_low)
        s_local[vs, :] = state
        s_send[vs, :] = bf(state)

    settle(z_note.at[0:96], n_sem, 1)
    all_to_all(state_out)
    s_recv[me] = s_send[own_state, :]
    d_recv[me] = d_send[me // 16]
    for c in range(1, CHUNKS):
        fill_z(c)
        send_z(c)
    got = z_note[...].astype(jnp.float32)
    token_row = lax.broadcasted_iota(jnp.int32, (128, 1), 0)
    offset = lax.shift_right_logical(token_row, 5) * 4
    live = got[:, 8:9] > 0.5
    slot_a = jnp.where(live, got[:, 0:1].astype(jnp.int32) + offset, -1)
    slot_b = jnp.where(live, got[:, 1:2].astype(jnp.int32) + offset, -1)
    slot_lane = lax.broadcasted_iota(jnp.int32, (128, 256), 1)
    place_a = bf(ones_where(slot_lane == slot_a))
    place_b = bf(ones_where(slot_lane == slot_b))
    place = place_a + place_b
    weight_a = got[:, 2:3] + got[:, 3:4] + got[:, 4:5]
    weight_b = got[:, 5:6] + got[:, 6:7] + got[:, 7:8]

    for c in range(CHUNKS):
        settle(z_recv.at[c, 0:96], z_sem.at[c], 1)
        x_send[c, :, :WIDE] = bf(dot_rows(place, z_recv[c, :, :WIDE]))
        cot_part = z_recv[c, :, WIDE:].astype(jnp.float32)
        x_send[c, :, WIDE:] = bf(
            dot_rows(place_a, bf(weight_a * cot_part)) + dot_rows(place_b, bf(weight_b * cot_part))
        )
        for dy, dx in PLANE:
            there = rows_at((ring(y, dy) * 4 + ring(x, dx)) * 16, 16)
            remote(
                x_send.at[c, there],
                rows.at[c, rows_at(mine + here * 16, 16)],
                x_sem.at[c],
                plane_peer(dy, dx),
            )
        rows[c, rows_at(mine + here * 16, 16), :] = x_send[c, own_x, :]
        if c == 1:
            settle(s_recv.at[0:63], s_sem, 1)
            settle(d_recv.at[0:63], e_sem, 1)
            d_factor[...] = jnp.exp(d_recv[...])
            scan(s_recv, s_back, False)
            all_to_all(state_in)
            s_in[own_state, :] = s_back[me]

    for h in range(4):
        ks = slice(h * DK, (h + 1) * DK)
        running = run_log[:, ks]
        middle = running[63:64]
        q_scaled = q_ref[:, ks].astype(jnp.float32) * DK ** (-0.5)
        q_near[:, ks] = q_scaled * jnp.exp(running - middle)
        k_near[:, ks] = k_ref[:, ks].astype(jnp.float32) * jnp.exp(middle - running)
        q_start[:, ks] = q_scaled * jnp.exp(running)
        scores[h] = jnp.where(upto, thrice(dot_cols, q_near[:, ks], k_near[:, ks]), 0.0)
    settle(s_in.at[0:1008], i_sem, 1)
    for h in range(4):
        ks = slice(h * DK, (h + 1) * DK)
        vs = slice(h * DV, (h + 1) * DV)
        raw = twice(dot, scores[h], v_ref[:, vs]) + twice(dot_cols, q_start[:, ks], s_in[vs, :])
        inverse = lax.rsqrt(jnp.mean(raw * raw, axis=-1, keepdims=True) + epsilon)
        normed[:, vs] = raw * inverse
        root[:, h : h + 1] = inverse
        n_all[rows_at(z * 128, 128), vs] = bf(raw * inverse)
    own_n = n_all.at[rows_at(z * 128, 128)]
    for dz in (2, 1, 3):
        remote(own_n, own_n, nz_sem, z_peer(dz))

    for load in loads[6:]:
        load.wait()
    their_rows = rows_at(other * 256, 256)
    own_rows = rows_at(mine, 256)

    def gather_up(c, part):
        cut = slice(c * WIDE, (c + 1) * WIDE)
        for ref, value in (
            (pre_gate, dot(rows[c, part, :WIDE], gate_w[cut, :])),
            (pre_up, dot(rows[c, part, :WIDE], up_w[cut, :])),
            (back_hidden, dot_cols(rows[c, part, WIDE:], down_w[:, cut])),
        ):
            ref[part, :] = value if c == 0 else ref[part, :] + value

    for c in range(CHUNKS):
        settle(rows.at[c, 0:240], x_sem.at[c], 1)
        remote(rows.at[c, own_rows], rows.at[c, own_rows], d_sem.at[c], partner)
        gather_up(c, own_rows)
        settle(rows.at[c, 0:256], d_sem.at[c], 1)
        gather_up(c, their_rows)

    gate_swish, gate_slope = silu_parts(pre_gate[...])
    hidden[...] = bf(gate_swish * pre_up[...])
    back_gate[...] = bf(back_hidden[...] * pre_up[...] * gate_slope)
    back_up[...] = bf(back_hidden[...] * gate_swish)

    def half_of(part, c):
        cut = slice(c * WIDE, (c + 1) * WIDE)
        return bf(
            dot_cols(back_gate[part, :], gate_w[cut, :]) + dot_cols(back_up[part, :], up_w[cut, :])
        )

    def send_half(c):
        half_send[c] = half_of(their_rows, c)
        remote(half_send.at[c], half_recv.at[c], h_sem.at[c], partner)

    def give_back(c):
        own_half = half_of(own_rows, c).astype(jnp.float32)
        settle(half_recv.at[c], h_sem.at[c], 1)
        ret_send[c] = bf(own_half + half_recv[c].astype(jnp.float32))
        for dy, dx in PLANE:
            there = rows_at((ring(y, dy) * 4 + ring(x, dx)) * 16, 16)
            remote(ret_send.at[c, there], ret_recv.at[c, own_x], r_sem.at[c], plane_peer(dy, dx))
        ret_recv[c, own_x, :] = ret_send[c, own_x, :]

    send_half(0)
    for c in range(CHUNKS):
        if c + 1 < CHUNKS:
            send_half(c + 1)
        give_back(c)

    for c in range(CHUNKS):
        cut = slice(c * WIDE, (c + 1) * WIDE)
        gate_out[0, cut, :] = bf(dot_rows(rows[c, :, :WIDE], back_gate[...]))
        up_out[0, cut, :] = bf(dot_rows(rows[c, :, :WIDE], back_up[...]))
        down_out[0, :, cut] = bf(dot_rows(hidden[...], rows[c, :, WIDE:]))

    own_tokens = rows_at(tp * 64, 64)

    def to_tokens(c):
        settle(ret_recv.at[c, 0:240], r_sem.at[c], 1)
        tok_send[c] = bf(z_recv[c, :, WIDE:].astype(jnp.float32) + dot(place, ret_recv[c]))
        for dz in (2, 1, 3):
            there = rows_at(ring(z, dz) * 32, 32)
            remote(tok_send.at[c, there], tok_recv.at[c, own_z], t_sem.at[c], z_peer(dz))
        tok_recv[c, own_z, :] = tok_send[c, own_z, :]

    def share_tokens(c):
        settle(tok_recv.at[c, 0:96], t_sem.at[c], 1)
        token_all[c, own_tokens, :] = bf(dot_rows(z_pick, tok_recv[c]))
        part = token_all.at[c, own_tokens]
        remote(part, part, a_sem.at[c], partner)

        @pl.when(z != c)
        def send():
            remote(part, tz.at[rows_at(z * 128 + tp * 64, 64)], tz_sem, (c, y, x, tp))

    def use_tokens(c, total):
        settle(token_all.at[c, 0:64], a_sem.at[c], 1)
        value = dot(token_all[c], out_w[c * WIDE : (c + 1) * WIDE, :])
        return value if total is None else total + value

    to_tokens(0)
    to_tokens(1)
    share_tokens(0)
    to_tokens(2)
    share_tokens(1)
    to_tokens(3)
    share_tokens(2)
    back_normed = use_tokens(0, None)
    back_normed = use_tokens(1, back_normed)
    share_tokens(3)
    back_normed = use_tokens(2, back_normed)
    back_normed = use_tokens(3, back_normed)

    for h in range(4):
        ks = slice(h * DK, (h + 1) * DK)
        vs = slice(h * DV, (h + 1) * DV)
        back = back_normed[:, vs]
        head_normed = normed[:, vs]
        back = root[:, h : h + 1] * (
            back - head_normed * jnp.mean(back * head_normed, axis=-1, keepdims=True)
        )
        normed[:, vs] = back
        b_send[vs, :] = bf(thrice(dot_rows, back, q_start[:, ks]))
    all_to_all(grad_out)
    b_recv[me] = b_send[own_state, :]

    tz[rows_at(z * 128, 128), :] = token_all[z]
    settle(tz.at[0:192], tz_sem, 1)
    for d in (1, 2, 3):
        part = tz.at[rows_at(along_z[d] * 128 + tp * 64, 64)]
        remote(part, part, tz2_sem, partner)
    settle(tz.at[0:192], tz2_sem, 1)
    settle(n_all.at[0:384], nz_sem, 1)
    o_send[...] = bf(dot_rows(tz[...], n_all[:, :512]))
    for d in (2, 1, 3):
        there = rows_at(along_y[d] * 128, 128)
        remote(o_send.at[there], o_recv.at[y], o_sem, (z, along_y[d], x, tp))
    o_recv[y] = o_send[rows_at(y * 128, 128), :]
    p_send[...] = bf(dot_rows(tz[...], n_all[:, 512:]))
    for d in (2, 1, 3):
        for j in range(4):
            there = rows_at(along_x[d] * 32 + j * 128, 32)
            remote(
                p_send.at[there], p_recv.at[x, j * 32 : (j + 1) * 32], p_sem, (z, y, along_x[d], tp)
            )
    for j in range(4):
        p_recv[x, j * 32 : (j + 1) * 32, :] = p_send[rows_at(x * 32 + j * 128, 32), :]
    settle(b_recv.at[0:63], b_sem, 1)
    scan(b_recv, b_back, True)
    all_to_all(grad_in)
    f_in[own_state, :] = b_back[me]

    for h in range(4):
        ks = slice(h * DK, (h + 1) * DK)
        vs = slice(h * DV, (h + 1) * DV)
        back = normed[:, vs]
        running = run_log[:, ks]
        middle = running[63:64]
        dots = jnp.where(upto, twice(dot_cols, back, v_ref[:, vs]), 0.0)
        q_back = jnp.exp(running - middle) * thrice(dot, dots, k_near[:, ks])
        q_back = q_back + jnp.exp(running) * twice(dot, back, s_in[vs, :])
        k_near[:, ks] = jnp.exp(middle - running) * thrice(dot_rows, dots, q_near[:, ks])
        normed[:, vs] = thrice(dot_rows, scores[h], back)
        q_near[:, ks] = q_back
        q_out[:, ks] = bf(q_back * DK ** (-0.5))
        s_local[vs, :] = jnp.exp(running[127:128]) * s_in[vs, :].astype(jnp.float32) + s_local[vs, :]

    settle(o_recv.at[0:3], o_sem, 1)
    o_part[...] = bf(total_of(o_recv))
    for d in (2, 1, 3):
        there = rows_at(along_x[d] * 32, 32)
        remote(o_part.at[there], o_last.at[x], o2_sem, (z, y, along_x[d], tp))
    o_last[x] = o_part[rows_at(x * 32, 32), :]
    settle(p_recv.at[0:3], p_sem, 1)
    p_part[...] = bf(total_of(p_recv))
    for d in (2, 1, 3):
        there = rows_at(along_y[d] * 32, 32)
        remote(p_part.at[there], p_last.at[y], p2_sem, (z, along_y[d], x, tp))
    p_last[y] = p_part[rows_at(y * 32, 32), :]
    settle(z_note_send.at[0:96], n_sem, 0)
    settle(s_send.at[0:1008], s_sem, 0)
    settle(d_recv.at[0:63], e_sem, 0)
    settle(s_back.at[0:63], i_sem, 0)
    settle(n_all.at[0:384], nz_sem, 0)
    settle(tz.at[0:192], tz_sem, 0)
    settle(tz.at[0:192], tz2_sem, 0)
    settle(b_send.at[0:1008], b_sem, 0)
    for c in range(CHUNKS):
        settle(z_send.at[c, 0:96], z_sem.at[c], 0)
        settle(x_send.at[c, 0:240], x_sem.at[c], 0)
        settle(rows.at[c, 0:256], d_sem.at[c], 0)
        settle(half_send.at[c], h_sem.at[c], 0)
        settle(ret_send.at[c, 0:240], r_sem.at[c], 0)
        settle(tok_send.at[c, 0:96], t_sem.at[c], 0)
        settle(token_all.at[c, 0:64], a_sem.at[c], 0)
    settle(f_in.at[0:1008], f_sem, 1)
    for h in range(4):
        ks = slice(h * DK, (h + 1) * DK)
        vs = slice(h * DV, (h + 1) * DV)
        running = run_log[:, ks]
        total = running[127:128]
        future = f_in[vs, :]
        k_back = k_near[:, ks] + jnp.exp(total - running) * dot(v_ref[:, vs], future)
        k_out[:, ks] = bf(k_back)
        v_out[:, vs] = bf(normed[:, vs] + twice(dot_cols, k_end[:, ks], future))
        cross = jnp.sum(s_local[vs, :] * future.astype(jnp.float32), axis=0, keepdims=True)
        q_scaled = q_ref[:, ks].astype(jnp.float32) * DK ** (-0.5)
        change = q_scaled * q_near[:, ks] - k_ref[:, ks].astype(jnp.float32) * k_back
        high, mid, low = pieces_of(change)
        within = dot(upper, bf(high)) + dot(upper, bf(mid)) + dot(upper, bf(low))
        decay_out[:, ks] = within + cross

    settle(o_last.at[0:3], o2_sem, 1)
    settle(p_last.at[0:3], p2_sem, 1)
    out_out[:, :512] = total_of(o_last)
    out_out[:, 512:] = total_of(p_last)
    settle(o_recv.at[0:3], o_sem, 0)
    settle(p_recv.at[0:3], p_sem, 0)
    settle(o_last.at[0:3], o2_sem, 0)
    settle(p_last.at[0:3], p2_sem, 0)
    settle(b_back.at[0:63], f_sem, 0)


def finish_kernel(*refs):
    count = len(refs) // 2
    sems = refs[-1]
    copies = []
    for n in range(count):
        copy = pltpu.make_async_copy(refs[n], refs[count + n], sems.at[n])
        copy.start()
        copies.append(copy)
    for copy in copies:
        copy.wait()


def whole_layer(experts, weights, mid, cot, gate, up, down, out_w, queries, keys, values, decay):
    b16, f32 = jnp.bfloat16, jnp.float32
    v = pltpu.VMEM
    dma = pltpu.SemaphoreType.DMA
    vmem = pl.BlockSpec(memory_space=pltpu.VMEM)
    hbm = pl.BlockSpec(memory_space=pl.ANY)
    outs = (
        ((1, 2048, 512), b16),
        ((1, 2048, 512), b16),
        ((1, 512, 2048), b16),
        ((32, 1024), f32),
        ((128, 512), b16),
        ((128, 512), b16),
        ((128, 1024), b16),
        ((128, 512), f32),
    )
    scratch = (
        ((64, 2048), b16),
        ((64, 2048), b16),
        ((2048, 512), b16),
        ((2048, 512), b16),
        ((512, 2048), b16),
        ((2048, 1024), b16),
        ((128, 512), b16),
        ((128, 512), b16),
        ((128, 1024), b16),
        ((128, 512), f32),
        ((CHUNKS, 128, 2 * WIDE), b16),
        ((128, 128), b16),
        ((CHUNKS, 128, 2 * WIDE), b16),
        ((128, 128), b16),
        ((CHUNKS, 256, 2 * WIDE), b16),
        ((CHUNKS, 512, 2 * WIDE), b16),
        ((512, 512), f32),
        ((512, 512), f32),
        ((512, 512), f32),
        ((512, 512), b16),
        ((512, 512), b16),
        ((512, 512), b16),
        ((CHUNKS, 256, WIDE), b16),
        ((CHUNKS, 256, WIDE), b16),
        ((CHUNKS, 256, WIDE), b16),
        ((CHUNKS, 256, WIDE), b16),
        ((CHUNKS, 128, WIDE), b16),
        ((CHUNKS, 128, WIDE), b16),
        ((4, 128, 512), b16),
        ((128, 512), f32),
        ((128, 512), f32),
        ((128, 512), f32),
        ((128, 512), f32),
        ((128, 512), f32),
        ((4, 128, 128), f32),
        ((128, 1024), f32),
        ((128, 128), f32),
        ((1024, 128), f32),
        ((1024, 128), b16),
        ((64, 16, 128), b16),
        ((64, 16, 128), b16),
        ((1024, 128), b16),
        ((4, 1, 128), f32),
        ((64, 1, 128), f32),
        ((64, 1, 128), f32),
        ((512, 1024), b16),
        ((1024, 128), b16),
        ((64, 16, 128), b16),
        ((64, 16, 128), b16),
        ((1024, 128), b16),
        ((512, 512), b16),
        ((512, 512), b16),
        ((4, 128, 512), b16),
        ((128, 512), b16),
        ((4, 32, 512), b16),
        ((512, 512), b16),
        ((4, 128, 512), b16),
        ((128, 512), b16),
        ((4, 32, 512), b16),
    )
    two, many = (2,), (CHUNKS, 2)
    sems = [(10,), two] + [many] * 7 + [two] * 12
    made = pl.pallas_call(
        layer_kernel,
        name="whole_layer",
        out_shape=tuple(v(shape, kind) for shape, kind in outs),
        in_specs=[vmem] * 2 + [hbm] * 10,
        out_specs=(vmem,) * 8,
        scratch_shapes=[v(shape, kind) for shape, kind in scratch] + [dma(shape) for shape in sems],
        compiler_params=pltpu.CompilerParams(
            collective_id=0, has_side_effects=True, vmem_limit_bytes=50 * 1024 * 1024
        ),
        cost_estimate=pl.CostEstimate(
            flops=11_000_000_000, bytes_accessed=20_000_000, transcendentals=600_000
        ),
    )(experts.T, weights.T, mid, cot, gate, up, down, out_w, queries, keys, values, decay)
    return pl.pallas_call(
        finish_kernel,
        name="finish",
        out_shape=tuple(jax.ShapeDtypeStruct(shape, kind) for shape, kind in outs),
        in_specs=[vmem] * 8,
        out_specs=(hbm,) * 8,
        scratch_shapes=[dma((8,))],
        compiler_params=pltpu.CompilerParams(vmem_limit_bytes=1024 * 1024),
    )(*[pltpu.with_memory_space_constraint(a, pltpu.VMEM) for a in made])


def body(
    mid_rows,
    cotangent,
    route_experts,
    route_weights,
    gate_weight,
    up_weight,
    down_weight,
    out_weight,
    queries,
    key_rows,
    value_rows,
    log_decay,
):
    return whole_layer(
        route_experts,
        route_weights,
        mid_rows,
        cotangent,
        gate_weight,
        up_weight,
        down_weight,
        out_weight,
        queries,
        key_rows,
        value_rows,
        log_decay,
    )


def solution(mesh):
    split = Mesh(mesh.devices.reshape(4, 4, 4, mesh.shape["tp"]), ("sp_0", "sp_1", "sp_2", "tp"))
    placed = (
        P(SP_TP, None),
        P(SP_TP, None),
        P(SP_TP, None),
        P(SP_TP, None),
        P(SP, None, "tp"),
        P(SP, None, "tp"),
        P(SP, "tp", None),
        P(None, "tp"),
        P(SP, "tp"),
        P(SP, "tp"),
        P(SP, "tp"),
        P(SP, "tp"),
    )
    return jax.shard_map(
        body,
        mesh=split,
        in_specs=placed,
        out_specs=(
            P(SP, None, "tp"),
            P(SP, None, "tp"),
            P(SP, "tp", None),
            P(SP, "tp"),
            P(SP, "tp"),
            P(SP, "tp"),
            P(SP, "tp"),
            P(SP, "tp"),
        ),
        check_vma=False,
    )
```

```python
import jax
import jax.numpy as jnp
from jax import lax
from jax.experimental import pallas as pl
from jax.experimental.pallas import tpu as pltpu
from jax.sharding import Mesh
from jax.sharding import PartitionSpec as P

DK = 128
DV = 256
SP = ("sp_0", "sp_1", "sp_2")
SP_TP = ("sp_0", "sp_1", "sp_2", "tp")
MESH = pl.DeviceIdType.MESH


epsilon = 1e-06
contract_rows = (((0,), (0,)), ((), ()))
contract_cols = (((1,), (1,)), ((), ()))


def silu_parts(pre_gate):
    gate_sigmoid = jax.nn.sigmoid(pre_gate)
    gate_swish = pre_gate * gate_sigmoid
    gate_slope = gate_sigmoid * (1.0 + pre_gate * (1.0 - gate_sigmoid))
    return (gate_swish, gate_slope)


def ring(base, step):
    return lax.rem(base + step, 4)


def rows_at(start, size):
    return pl.ds(pl.multiple_of(start, size), size)


def dot(a, b):
    return lax.dot_general(a, b, (((1,), (0,)), ((), ())), preferred_element_type=jnp.float32)


def dot_rows(a, b):
    return lax.dot_general(a, b, contract_rows, preferred_element_type=jnp.float32)


def dot_cols(a, b):
    return lax.dot_general(a, b, contract_cols, preferred_element_type=jnp.float32)


def ones_where(mask):
    return jnp.where(mask, 1.0, 0.0).astype(jnp.float32)


def bf(a):
    return a.astype(jnp.bfloat16)


def total_of(parts):
    total = parts[0].astype(jnp.float32) + parts[1].astype(jnp.float32)
    return total + parts[2].astype(jnp.float32) + parts[3].astype(jnp.float32)


def pieces_of(a):
    high = bf(a).astype(jnp.float32)
    mid = bf(a - high).astype(jnp.float32)
    return high, mid, a - high - mid


def split(a):
    high = bf(a)
    return high, bf(a - high.astype(jnp.float32))


def twice(f, a, b):
    high, low = split(a)
    return f(high, b) + f(low, b)


def thrice(f, a, b):
    a_high, a_low = split(a)
    b_high, b_low = split(b)
    return f(a_high, b_high) + (f(a_high, b_low) + f(a_low, b_high))


PLANE = sorted(
    [(dy, dx) for dy in range(4) for dx in range(4) if (dy, dx) != (0, 0)],
    key=lambda o: -(min(o[0], 4 - o[0]) + min(o[1], 4 - o[1])),
)
FAR = sorted(
    [(i, j, k) for i in range(4) for j in range(4) for k in range(4) if i + j + k],
    key=lambda o: -sum(min(d, 4 - d) for d in o),
)
CHUNKS = 4
WIDE = 2048 // CHUNKS
ORDER = [4 * place + c for c in range(CHUNKS) for place in range(4)]
BOUNDS = (0, 2, 6, 10, 14, 16)
STEPS = tuple(zip(BOUNDS[:-1], BOUNDS[1:]))
LANES = 128


def block_of(p):
    return slice(ORDER[p] * LANES, (ORDER[p] + 1) * LANES)


def taken_columns(ref, low, high):
    return jnp.concatenate([ref[:, block_of(p)] for p in range(low, high)], axis=1)


def taken_rows(ref, low, high):
    return jnp.concatenate([ref[block_of(p), :] for p in range(low, high)], axis=0)


def mid_part(low, high):
    return slice(2 * low * LANES, (low + high) * LANES)


def cot_part_of(low, high):
    return slice((low + high) * LANES, 2 * high * LANES)


def both_parts(low, high):
    return slice(2 * low * LANES, 2 * high * LANES)


def cot_block(p):
    low, high = [step for step in STEPS if step[0] <= p < step[1]][0]
    at = low + high + p - low
    return slice(at * LANES, (at + 1) * LANES)


def layer_kernel(
    experts_ref,
    weights_ref,
    mid_hbm,
    cot_hbm,
    gate_hbm,
    up_hbm,
    down_hbm,
    out_w_hbm,
    q_hbm,
    k_hbm,
    v_hbm,
    decay_hbm,
    gate_out,
    up_out,
    down_out,
    out_out,
    q_out,
    k_out,
    v_out,
    decay_out,
    mid_ref,
    cot_ref,
    gate_w,
    up_w,
    down_w,
    out_w,
    q_ref,
    k_ref,
    v_ref,
    decay_ref,
    z_send,
    z_note_send,
    z_recv,
    z_note,
    x_send,
    rows,
    pre_gate,
    pre_up,
    back_hidden,
    hidden,
    back_gate,
    back_up,
    half_send,
    half_recv,
    ret_send,
    ret_recv,
    tok_send,
    tok_recv,
    token_all,
    run_log,
    q_near,
    k_near,
    q_start,
    k_end,
    scores,
    normed,
    root,
    s_local,
    s_send,
    s_recv,
    s_back,
    s_in,
    d_send,
    d_recv,
    d_factor,
    n_all,
    b_send,
    b_recv,
    b_back,
    f_in,
    tz,
    o_send,
    o_recv,
    o_part,
    o_last,
    p_send,
    p_recv,
    p_part,
    p_last,
    w_sem,
    n_sem,
    z_sem,
    x_sem,
    d_sem,
    h_sem,
    r_sem,
    t_sem,
    a_sem,
    s_sem,
    e_sem,
    i_sem,
    b_sem,
    f_sem,
    nz_sem,
    tz_sem,
    tz2_sem,
    o_sem,
    o2_sem,
    p_sem,
    p2_sem,
):
    z, y, x, tp = [lax.axis_index(a) for a in SP_TP]
    other = 1 - tp
    here = y * 4 + x
    me = z * 16 + here
    mine = tp * 256

    def z_peer(dz):
        return (ring(z, dz), y, x, tp)

    def plane_peer(dy, dx):
        return (z, ring(y, dy), ring(x, dx), tp)

    partner = (z, y, x, other)
    barrier = pltpu.get_barrier_semaphore()
    peers = [z_peer(dz) for dz in (2, 1, 3)] + [plane_peer(*o) for o in PLANE] + [partner]
    for peer in peers:
        pl.semaphore_signal(barrier, inc=1, device_id=peer, device_id_type=MESH)

    loads = []
    moved = (
        (mid_hbm, mid_ref),
        (cot_hbm, cot_ref),
        (decay_hbm, decay_ref),
        (k_hbm, k_ref),
        (v_hbm, v_ref),
        (q_hbm, q_ref),
        (gate_hbm.at[0], gate_w),
        (up_hbm.at[0], up_w),
        (down_hbm.at[0], down_w),
        (out_w_hbm, out_w),
    )
    for n, (src, dst) in enumerate(moved):
        load = pltpu.make_async_copy(src, dst, w_sem.at[n])
        load.start()
        loads.append(load)

    def remote(src, dst, sem, peer):
        copy = pltpu.make_async_remote_copy(
            src_ref=src,
            dst_ref=dst,
            send_sem=sem.at[0],
            recv_sem=sem.at[1],
            device_id=peer,
            device_id_type=MESH,
        )
        copy.start()

    def settle(ref, sem, side):
        pltpu.make_async_copy(ref, ref, sem.at[side]).wait()

    first = experts_ref[0:1, :]
    second = experts_ref[1:2, :]
    expert_row = lax.broadcasted_iota(jnp.int32, (64, 64), 0)
    token_lane = lax.broadcasted_iota(jnp.int32, (64, 64), 1)
    named_first = ones_where(expert_row == first)
    named_second = ones_where(expert_row == second)
    before = bf(ones_where(expert_row < token_lane))
    counts = dot(bf(named_first + named_second), before)
    rank_first = jnp.sum(named_first * counts, axis=0, keepdims=True)
    rank_second = jnp.sum(named_second * counts, axis=0, keepdims=True)
    group = lax.shift_right_logical(first, 4)
    in_group = ones_where(expert_row[:16] == group)
    group_rank = jnp.sum(in_group * dot(bf(in_group), before), axis=0, keepdims=True)
    z_slot = group * 32 + group_rank.astype(jnp.int32)
    slot_row = lax.broadcasted_iota(jnp.int32, (128, 64), 0)
    z_pick = bf(ones_where(slot_row == z_slot))
    slot_first = (jnp.bitwise_and(first, 15) * 16).astype(jnp.float32) + rank_first
    slot_second = (jnp.bitwise_and(second, 15) * 16).astype(jnp.float32) + rank_second
    columns = [slot_first, slot_second]
    columns += list(pieces_of(weights_ref[0:1, :])) + list(pieces_of(weights_ref[1:2, :]))
    note = ones_where(slot_row == 8)
    for n, column in enumerate(columns):
        note = jnp.where(slot_row == n, column, note)
    z_note_send[...] = bf(dot_cols(z_pick, bf(note)))
    own_z = rows_at(z * 32, 32)
    own_x = rows_at(here * 16, 16)

    loads[0].wait()
    loads[1].wait()

    def fill_z(n):
        z_send[:, mid_part(*STEPS[n])] = bf(dot(z_pick, taken_columns(mid_ref, *STEPS[n])))
        z_send[:, cot_part_of(*STEPS[n])] = bf(dot(z_pick, taken_columns(cot_ref, *STEPS[n])))

    fill_z(0)
    pl.semaphore_wait(barrier, len(peers))

    for dz in (2, 1, 3):
        there = rows_at(ring(z, dz) * 32, 32)
        remote(z_note_send.at[there], z_note.at[own_z], n_sem, z_peer(dz))
    z_note[own_z, :] = z_note_send[own_z, :]

    def send_z(n):
        part = both_parts(*STEPS[n])
        for dz in (2, 1, 3):
            there = rows_at(ring(z, dz) * 32, 32)
            remote(z_send.at[there, part], z_recv.at[own_z, part], z_sem.at[n], z_peer(dz))
        z_recv[own_z, part] = z_send[own_z, part]

    send_z(0)
    fill_z(1)
    send_z(1)

    along_z, along_y, along_x = [[ring(a, d) for d in range(4)] for a in (z, y, x)]
    bases = [[along_z[i] * 16 + along_y[j] * 4 for j in range(4)] for i in range(4)]

    def all_to_all(send):
        for i, j, k in FAR:
            peer = (along_z[i], along_y[j], along_x[k], tp)
            send(peer, bases[i][j] + along_x[k])

    def state_out(peer, there):
        remote(s_send.at[rows_at(there * 16, 16)], s_recv.at[me], s_sem, peer)
        remote(d_send.at[there // 16], d_recv.at[me], e_sem, peer)

    def state_in(peer, there):
        remote(s_back.at[there], s_in.at[own_state], i_sem, peer)

    def grad_out(peer, there):
        remote(b_send.at[rows_at(there * 16, 16)], b_recv.at[me], b_sem, peer)

    def grad_in(peer, there):
        remote(b_back.at[there], f_in.at[own_state], f_sem, peer)

    def scan(recv, back, reverse):
        state = jnp.zeros((16, DK), jnp.float32)
        for n in range(64):
            at = 63 - n if reverse else n
            back[at] = bf(state)
            state = d_factor[at] * state + recv[at].astype(jnp.float32)

    own_state = rows_at(me * 16, 16)
    square = (128, 128)
    at_row = lax.broadcasted_iota(jnp.int32, square, 0)
    at_col = lax.broadcasted_iota(jnp.int32, square, 1)
    upto = at_row >= at_col
    lower = bf(ones_where(upto))
    upper = bf(ones_where(at_row <= at_col))
    for load in loads[2:6]:
        load.wait()
    high, mid, low = pieces_of(decay_ref[...])
    run_log[...] = dot(lower, bf(high)) + dot(lower, bf(mid)) + dot(lower, bf(low))
    for h in range(4):
        ks = slice(h * DK, (h + 1) * DK)
        vs = slice(h * DV, (h + 1) * DV)
        running = run_log[:, ks]
        total = running[127:128]
        d_send[h] = total
        k_end[:, ks] = k_ref[:, ks].astype(jnp.float32) * jnp.exp(total - running)
        k_high, k_low = split(k_end[:, ks])
        state = dot_rows(v_ref[:, vs], k_high) + dot_rows(v_ref[:, vs], k_low)
        s_local[vs, :] = state
        s_send[vs, :] = bf(state)

    settle(z_note.at[0:96], n_sem, 1)
    all_to_all(state_out)
    s_recv[me] = s_send[own_state, :]
    d_recv[me] = d_send[me // 16]
    for n in range(2, len(STEPS)):
        fill_z(n)
        send_z(n)
    got = z_note[...].astype(jnp.float32)
    token_row = lax.broadcasted_iota(jnp.int32, (128, 1), 0)
    offset = lax.shift_right_logical(token_row, 5) * 4
    live = got[:, 8:9] > 0.5
    slot_a = jnp.where(live, got[:, 0:1].astype(jnp.int32) + offset, -1)
    slot_b = jnp.where(live, got[:, 1:2].astype(jnp.int32) + offset, -1)
    slot_lane = lax.broadcasted_iota(jnp.int32, (128, 256), 1)
    place_a = bf(ones_where(slot_lane == slot_a))
    place_b = bf(ones_where(slot_lane == slot_b))
    place = place_a + place_b
    weight_a = got[:, 2:3] + got[:, 3:4] + got[:, 4:5]
    weight_b = got[:, 5:6] + got[:, 6:7] + got[:, 7:8]

    for c, step in enumerate(STEPS):
        settle(z_recv.at[0:96, both_parts(*step)], z_sem.at[c], 1)
        x_send[:, mid_part(*step)] = bf(dot_rows(place, z_recv[:, mid_part(*step)]))
        cot_part = z_recv[:, cot_part_of(*step)].astype(jnp.float32)
        x_send[:, cot_part_of(*step)] = bf(
            dot_rows(place_a, bf(weight_a * cot_part)) + dot_rows(place_b, bf(weight_b * cot_part))
        )
        part = both_parts(*step)
        for dy, dx in PLANE:
            there = rows_at((ring(y, dy) * 4 + ring(x, dx)) * 16, 16)
            remote(
                x_send.at[there, part],
                rows.at[rows_at(mine + here * 16, 16), part],
                x_sem.at[c],
                plane_peer(dy, dx),
            )
        rows[rows_at(mine + here * 16, 16), part] = x_send[own_x, part]
        if c == 1:
            settle(s_recv.at[0:63], s_sem, 1)
            settle(d_recv.at[0:63], e_sem, 1)
            d_factor[...] = jnp.exp(d_recv[...])
            scan(s_recv, s_back, False)
            all_to_all(state_in)
            s_in[own_state, :] = s_back[me]

    for h in range(4):
        ks = slice(h * DK, (h + 1) * DK)
        running = run_log[:, ks]
        middle = running[63:64]
        q_scaled = q_ref[:, ks].astype(jnp.float32) * DK ** (-0.5)
        q_near[:, ks] = q_scaled * jnp.exp(running - middle)
        k_near[:, ks] = k_ref[:, ks].astype(jnp.float32) * jnp.exp(middle - running)
        q_start[:, ks] = q_scaled * jnp.exp(running)
        scores[h] = jnp.where(upto, thrice(dot_cols, q_near[:, ks], k_near[:, ks]), 0.0)
    settle(s_in.at[0:1008], i_sem, 1)
    for h in range(4):
        ks = slice(h * DK, (h + 1) * DK)
        vs = slice(h * DV, (h + 1) * DV)
        raw = twice(dot, scores[h], v_ref[:, vs]) + twice(dot_cols, q_start[:, ks], s_in[vs, :])
        inverse = lax.rsqrt(jnp.mean(raw * raw, axis=-1, keepdims=True) + epsilon)
        normed[:, vs] = raw * inverse
        root[:, h : h + 1] = inverse
        n_all[rows_at(z * 128, 128), vs] = bf(raw * inverse)
    own_n = n_all.at[rows_at(z * 128, 128)]
    for dz in (2, 1, 3):
        remote(own_n, own_n, nz_sem, z_peer(dz))

    for load in loads[6:]:
        load.wait()
    their_rows = rows_at(other * 256, 256)
    own_rows = rows_at(mine, 256)

    def gather_up(c, part):
        step = STEPS[c]
        mid_rows = rows[part, mid_part(*step)]
        for ref, value in (
            (pre_gate, dot(mid_rows, taken_rows(gate_w, *step))),
            (pre_up, dot(mid_rows, taken_rows(up_w, *step))),
            (back_hidden, dot_cols(rows[part, cot_part_of(*step)], taken_columns(down_w, *step))),
        ):
            ref[part, :] = value if c == 0 else ref[part, :] + value

    for c, step in enumerate(STEPS):
        part = both_parts(*step)
        settle(rows.at[0:240, part], x_sem.at[c], 1)
        remote(rows.at[own_rows, part], rows.at[own_rows, part], d_sem.at[c], partner)
        gather_up(c, own_rows)
        settle(rows.at[0:256, part], d_sem.at[c], 1)
        gather_up(c, their_rows)

    gate_swish, gate_slope = silu_parts(pre_gate[...])
    hidden[...] = bf(gate_swish * pre_up[...])
    back_gate[...] = bf(back_hidden[...] * pre_up[...] * gate_slope)
    back_up[...] = bf(back_hidden[...] * gate_swish)

    def half_of(part, c):
        return bf(
            dot_cols(back_gate[part, :], taken_rows(gate_w, 4 * c, 4 * c + 4))
            + dot_cols(back_up[part, :], taken_rows(up_w, 4 * c, 4 * c + 4))
        )

    def send_half(c):
        half_send[c] = half_of(their_rows, c)
        remote(half_send.at[c], half_recv.at[c], h_sem.at[c], partner)

    def give_back(c):
        own_half = half_of(own_rows, c).astype(jnp.float32)
        settle(half_recv.at[c], h_sem.at[c], 1)
        ret_send[c] = bf(own_half + half_recv[c].astype(jnp.float32))
        for dy, dx in PLANE:
            there = rows_at((ring(y, dy) * 4 + ring(x, dx)) * 16, 16)
            remote(ret_send.at[c, there], ret_recv.at[c, own_x], r_sem.at[c], plane_peer(dy, dx))
        ret_recv[c, own_x, :] = ret_send[c, own_x, :]

    send_half(0)
    for c in range(CHUNKS):
        if c + 1 < CHUNKS:
            send_half(c + 1)
        give_back(c)

    for low, high in STEPS:
        mid_rows = rows[:, mid_part(low, high)]
        for out, grad in ((gate_out, back_gate), (up_out, back_up)):
            value = bf(dot_rows(mid_rows, grad[...]))
            for p in range(low, high):
                out[0, block_of(p), :] = value[(p - low) * LANES : (p - low + 1) * LANES, :]
        value = bf(dot_rows(hidden[...], rows[:, cot_part_of(low, high)]))
        for p in range(low, high):
            down_out[0, :, block_of(p)] = value[:, (p - low) * LANES : (p - low + 1) * LANES]

    own_tokens = rows_at(tp * 64, 64)

    def to_tokens(c):
        settle(ret_recv.at[c, 0:240], r_sem.at[c], 1)
        cot_rows = jnp.concatenate(
            [z_recv[:, cot_block(p)] for p in range(4 * c, 4 * c + 4)], axis=1
        )
        tok_send[c] = bf(cot_rows.astype(jnp.float32) + dot(place, ret_recv[c]))
        for dz in (2, 1, 3):
            there = rows_at(ring(z, dz) * 32, 32)
            remote(tok_send.at[c, there], tok_recv.at[c, own_z], t_sem.at[c], z_peer(dz))
        tok_recv[c, own_z, :] = tok_send[c, own_z, :]

    def share_tokens(c):
        settle(tok_recv.at[c, 0:96], t_sem.at[c], 1)
        token_all[c, own_tokens, :] = bf(dot_rows(z_pick, tok_recv[c]))
        part = token_all.at[c, own_tokens]
        remote(part, part, a_sem.at[c], partner)
        for d in (2, 1, 3):
            remote(
                token_all.at[c, own_tokens, rows_at(along_z[d] * LANES, LANES)],
                tz.at[rows_at(z * 128 + tp * 64, 64), c * LANES : (c + 1) * LANES],
                tz_sem,
                z_peer(d),
            )

    def use_tokens(c, total):
        settle(token_all.at[c, 0:64], a_sem.at[c], 1)
        value = dot(token_all[c], taken_rows(out_w, 4 * c, 4 * c + 4))
        return value if total is None else total + value

    to_tokens(0)
    to_tokens(1)
    share_tokens(0)
    to_tokens(2)
    share_tokens(1)
    to_tokens(3)
    share_tokens(2)
    back_normed = use_tokens(0, None)
    back_normed = use_tokens(1, back_normed)
    share_tokens(3)
    back_normed = use_tokens(2, back_normed)
    back_normed = use_tokens(3, back_normed)

    for h in range(4):
        ks = slice(h * DK, (h + 1) * DK)
        vs = slice(h * DV, (h + 1) * DV)
        back = back_normed[:, vs]
        head_normed = normed[:, vs]
        back = root[:, h : h + 1] * (
            back - head_normed * jnp.mean(back * head_normed, axis=-1, keepdims=True)
        )
        normed[:, vs] = back
        b_send[vs, :] = bf(thrice(dot_rows, back, q_start[:, ks]))
    all_to_all(grad_out)
    b_recv[me] = b_send[own_state, :]

    for c in range(CHUNKS):
        tz[rows_at(z * 128, 128), c * LANES : (c + 1) * LANES] = token_all[
            c, :, rows_at(z * LANES, LANES)
        ]
    settle(tz.at[0:192], tz_sem, 1)
    for d in (1, 2, 3):
        part = tz.at[rows_at(along_z[d] * 128 + tp * 64, 64)]
        remote(part, part, tz2_sem, partner)
    settle(tz.at[0:192], tz2_sem, 1)
    settle(n_all.at[0:384], nz_sem, 1)
    o_send[...] = bf(dot_rows(tz[...], n_all[:, :512]))
    for d in (2, 1, 3):
        there = rows_at(along_y[d] * 128, 128)
        remote(o_send.at[there], o_recv.at[y], o_sem, (z, along_y[d], x, tp))
    o_recv[y] = o_send[rows_at(y * 128, 128), :]
    p_send[...] = bf(dot_rows(tz[...], n_all[:, 512:]))
    for d in (2, 1, 3):
        for j in range(4):
            there = rows_at(along_x[d] * 32 + j * 128, 32)
            remote(
                p_send.at[there], p_recv.at[x, j * 32 : (j + 1) * 32], p_sem, (z, y, along_x[d], tp)
            )
    for j in range(4):
        p_recv[x, j * 32 : (j + 1) * 32, :] = p_send[rows_at(x * 32 + j * 128, 32), :]
    settle(b_recv.at[0:63], b_sem, 1)
    scan(b_recv, b_back, True)
    all_to_all(grad_in)
    f_in[own_state, :] = b_back[me]

    for h in range(4):
        ks = slice(h * DK, (h + 1) * DK)
        vs = slice(h * DV, (h + 1) * DV)
        back = normed[:, vs]
        running = run_log[:, ks]
        middle = running[63:64]
        dots = jnp.where(upto, twice(dot_cols, back, v_ref[:, vs]), 0.0)
        q_back = jnp.exp(running - middle) * thrice(dot, dots, k_near[:, ks])
        q_back = q_back + jnp.exp(running) * twice(dot, back, s_in[vs, :])
        k_near[:, ks] = jnp.exp(middle - running) * thrice(dot_rows, dots, q_near[:, ks])
        normed[:, vs] = thrice(dot_rows, scores[h], back)
        q_near[:, ks] = q_back
        q_out[:, ks] = bf(q_back * DK ** (-0.5))
        s_local[vs, :] = jnp.exp(running[127:128]) * s_in[vs, :].astype(jnp.float32) + s_local[vs, :]

    settle(o_recv.at[0:3], o_sem, 1)
    o_part[...] = bf(total_of(o_recv))
    for d in (2, 1, 3):
        there = rows_at(along_x[d] * 32, 32)
        remote(o_part.at[there], o_last.at[x], o2_sem, (z, y, along_x[d], tp))
    o_last[x] = o_part[rows_at(x * 32, 32), :]
    settle(p_recv.at[0:3], p_sem, 1)
    p_part[...] = bf(total_of(p_recv))
    for d in (2, 1, 3):
        there = rows_at(along_y[d] * 32, 32)
        remote(p_part.at[there], p_last.at[y], p2_sem, (z, along_y[d], x, tp))
    p_last[y] = p_part[rows_at(y * 32, 32), :]
    settle(z_note_send.at[0:96], n_sem, 0)
    settle(s_send.at[0:1008], s_sem, 0)
    settle(d_recv.at[0:63], e_sem, 0)
    settle(s_back.at[0:63], i_sem, 0)
    settle(n_all.at[0:384], nz_sem, 0)
    settle(tz.at[0:192], tz_sem, 0)
    settle(tz.at[0:192], tz2_sem, 0)
    settle(b_send.at[0:1008], b_sem, 0)
    for c, step in enumerate(STEPS):
        settle(z_send.at[0:96, both_parts(*step)], z_sem.at[c], 0)
        settle(x_send.at[0:240, both_parts(*step)], x_sem.at[c], 0)
        settle(rows.at[0:256, both_parts(*step)], d_sem.at[c], 0)
    for c in range(CHUNKS):
        settle(half_send.at[c], h_sem.at[c], 0)
        settle(ret_send.at[c, 0:240], r_sem.at[c], 0)
        settle(tok_send.at[c, 0:96], t_sem.at[c], 0)
        settle(token_all.at[c, 0:64], a_sem.at[c], 0)
    settle(f_in.at[0:1008], f_sem, 1)
    for h in range(4):
        ks = slice(h * DK, (h + 1) * DK)
        vs = slice(h * DV, (h + 1) * DV)
        running = run_log[:, ks]
        total = running[127:128]
        future = f_in[vs, :]
        k_back = k_near[:, ks] + jnp.exp(total - running) * dot(v_ref[:, vs], future)
        k_out[:, ks] = bf(k_back)
        v_out[:, vs] = bf(normed[:, vs] + twice(dot_cols, k_end[:, ks], future))
        cross = jnp.sum(s_local[vs, :] * future.astype(jnp.float32), axis=0, keepdims=True)
        q_scaled = q_ref[:, ks].astype(jnp.float32) * DK ** (-0.5)
        change = q_scaled * q_near[:, ks] - k_ref[:, ks].astype(jnp.float32) * k_back
        high, mid, low = pieces_of(change)
        within = dot(upper, bf(high)) + dot(upper, bf(mid)) + dot(upper, bf(low))
        decay_out[:, ks] = within + cross

    settle(o_last.at[0:3], o2_sem, 1)
    settle(p_last.at[0:3], p2_sem, 1)
    out_out[:, :512] = total_of(o_last)
    out_out[:, 512:] = total_of(p_last)
    settle(o_recv.at[0:3], o_sem, 0)
    settle(p_recv.at[0:3], p_sem, 0)
    settle(o_last.at[0:3], o2_sem, 0)
    settle(p_last.at[0:3], p2_sem, 0)
    settle(b_back.at[0:63], f_sem, 0)


def finish_kernel(*refs):
    count = len(refs) // 2
    sems = refs[-1]
    copies = []
    for n in range(count):
        copy = pltpu.make_async_copy(refs[n], refs[count + n], sems.at[n])
        copy.start()
        copies.append(copy)
    for copy in copies:
        copy.wait()


def whole_layer(experts, weights, mid, cot, gate, up, down, out_w, queries, keys, values, decay):
    b16, f32 = jnp.bfloat16, jnp.float32
    v = pltpu.VMEM
    dma = pltpu.SemaphoreType.DMA
    vmem = pl.BlockSpec(memory_space=pltpu.VMEM)
    hbm = pl.BlockSpec(memory_space=pl.ANY)
    outs = (
        ((1, 2048, 512), b16),
        ((1, 2048, 512), b16),
        ((1, 512, 2048), b16),
        ((32, 1024), f32),
        ((128, 512), b16),
        ((128, 512), b16),
        ((128, 1024), b16),
        ((128, 512), f32),
    )
    scratch = (
        ((64, 2048), b16),
        ((64, 2048), b16),
        ((2048, 512), b16),
        ((2048, 512), b16),
        ((512, 2048), b16),
        ((2048, 1024), b16),
        ((128, 512), b16),
        ((128, 512), b16),
        ((128, 1024), b16),
        ((128, 512), f32),
        ((128, 4096), b16),
        ((128, 128), b16),
        ((128, 4096), b16),
        ((128, 128), b16),
        ((256, 4096), b16),
        ((512, 4096), b16),
        ((512, 512), f32),
        ((512, 512), f32),
        ((512, 512), f32),
        ((512, 512), b16),
        ((512, 512), b16),
        ((512, 512), b16),
        ((CHUNKS, 256, WIDE), b16),
        ((CHUNKS, 256, WIDE), b16),
        ((CHUNKS, 256, WIDE), b16),
        ((CHUNKS, 256, WIDE), b16),
        ((CHUNKS, 128, WIDE), b16),
        ((CHUNKS, 128, WIDE), b16),
        ((4, 128, 512), b16),
        ((128, 512), f32),
        ((128, 512), f32),
        ((128, 512), f32),
        ((128, 512), f32),
        ((128, 512), f32),
        ((4, 128, 128), f32),
        ((128, 1024), f32),
        ((128, 128), f32),
        ((1024, 128), f32),
        ((1024, 128), b16),
        ((64, 16, 128), b16),
        ((64, 16, 128), b16),
        ((1024, 128), b16),
        ((4, 1, 128), f32),
        ((64, 1, 128), f32),
        ((64, 1, 128), f32),
        ((512, 1024), b16),
        ((1024, 128), b16),
        ((64, 16, 128), b16),
        ((64, 16, 128), b16),
        ((1024, 128), b16),
        ((512, 512), b16),
        ((512, 512), b16),
        ((4, 128, 512), b16),
        ((128, 512), b16),
        ((4, 32, 512), b16),
        ((512, 512), b16),
        ((4, 128, 512), b16),
        ((128, 512), b16),
        ((4, 32, 512), b16),
    )
    two, many, steps = (2,), (CHUNKS, 2), (len(STEPS), 2)
    sems = [(10,), two] + [steps] * 3 + [many] * 4 + [two] * 12
    made = pl.pallas_call(
        layer_kernel,
        name="whole_layer",
        out_shape=tuple(v(shape, kind) for shape, kind in outs),
        in_specs=[vmem] * 2 + [hbm] * 10,
        out_specs=(vmem,) * 8,
        scratch_shapes=[v(shape, kind) for shape, kind in scratch] + [dma(shape) for shape in sems],
        compiler_params=pltpu.CompilerParams(
            collective_id=0, has_side_effects=True, vmem_limit_bytes=50 * 1024 * 1024
        ),
        cost_estimate=pl.CostEstimate(
            flops=11_000_000_000, bytes_accessed=20_000_000, transcendentals=600_000
        ),
    )(experts.T, weights.T, mid, cot, gate, up, down, out_w, queries, keys, values, decay)
    return pl.pallas_call(
        finish_kernel,
        name="finish",
        out_shape=tuple(jax.ShapeDtypeStruct(shape, kind) for shape, kind in outs),
        in_specs=[vmem] * 8,
        out_specs=(hbm,) * 8,
        scratch_shapes=[dma((8,))],
        compiler_params=pltpu.CompilerParams(vmem_limit_bytes=1024 * 1024),
    )(*[pltpu.with_memory_space_constraint(a, pltpu.VMEM) for a in made])


def body(
    mid_rows,
    cotangent,
    route_experts,
    route_weights,
    gate_weight,
    up_weight,
    down_weight,
    out_weight,
    queries,
    key_rows,
    value_rows,
    log_decay,
):
    return whole_layer(
        route_experts,
        route_weights,
        mid_rows,
        cotangent,
        gate_weight,
        up_weight,
        down_weight,
        out_weight,
        queries,
        key_rows,
        value_rows,
        log_decay,
    )


def solution(mesh):
    split = Mesh(mesh.devices.reshape(4, 4, 4, mesh.shape["tp"]), ("sp_0", "sp_1", "sp_2", "tp"))
    placed = (
        P(SP_TP, None),
        P(SP_TP, None),
        P(SP_TP, None),
        P(SP_TP, None),
        P(SP, None, "tp"),
        P(SP, None, "tp"),
        P(SP, "tp", None),
        P(None, "tp"),
        P(SP, "tp"),
        P(SP, "tp"),
        P(SP, "tp"),
        P(SP, "tp"),
    )
    return jax.shard_map(
        body,
        mesh=split,
        in_specs=placed,
        out_specs=(
            P(SP, None, "tp"),
            P(SP, None, "tp"),
            P(SP, "tp", None),
            P(SP, "tp"),
            P(SP, "tp"),
            P(SP, "tp"),
            P(SP, "tp"),
            P(SP, "tp"),
        ),
        check_vma=False,
    )
```

```python
import jax
import jax.numpy as jnp
from jax import lax
from jax.experimental import pallas as pl
from jax.experimental.pallas import tpu as pltpu
from jax.sharding import Mesh
from jax.sharding import PartitionSpec as P

DK = 128
DV = 256
SP = ("sp_0", "sp_1", "sp_2")
SP_TP = ("sp_0", "sp_1", "sp_2", "tp")
MESH = pl.DeviceIdType.MESH


epsilon = 1e-06
contract_rows = (((0,), (0,)), ((), ()))
contract_cols = (((1,), (1,)), ((), ()))


def silu_parts(pre_gate):
    gate_sigmoid = jax.nn.sigmoid(pre_gate)
    gate_swish = pre_gate * gate_sigmoid
    gate_slope = gate_sigmoid * (1.0 + pre_gate * (1.0 - gate_sigmoid))
    return (gate_swish, gate_slope)


def ring(base, step):
    return lax.rem(base + step, 4)


def rows_at(start, size):
    return pl.ds(pl.multiple_of(start, size), size)


def dot(a, b):
    return lax.dot_general(a, b, (((1,), (0,)), ((), ())), preferred_element_type=jnp.float32)


def dot_rows(a, b):
    return lax.dot_general(a, b, contract_rows, preferred_element_type=jnp.float32)


def dot_cols(a, b):
    return lax.dot_general(a, b, contract_cols, preferred_element_type=jnp.float32)


def ones_where(mask):
    return jnp.where(mask, 1.0, 0.0).astype(jnp.float32)


def bf(a):
    return a.astype(jnp.bfloat16)


def total_of(parts):
    total = parts[0].astype(jnp.float32) + parts[1].astype(jnp.float32)
    return total + parts[2].astype(jnp.float32) + parts[3].astype(jnp.float32)


def pieces_of(a):
    high = bf(a).astype(jnp.float32)
    mid = bf(a - high).astype(jnp.float32)
    return high, mid, a - high - mid


def split(a):
    high = bf(a)
    return high, bf(a - high.astype(jnp.float32))


def twice(f, a, b):
    high, low = split(a)
    return f(high, b) + f(low, b)


def thrice(f, a, b):
    a_high, a_low = split(a)
    b_high, b_low = split(b)
    return f(a_high, b_high) + (f(a_high, b_low) + f(a_low, b_high))


PLANE = sorted(
    [(dy, dx) for dy in range(4) for dx in range(4) if (dy, dx) != (0, 0)],
    key=lambda o: -(min(o[0], 4 - o[0]) + min(o[1], 4 - o[1])),
)
FAR = sorted(
    [(i, j, k) for i in range(4) for j in range(4) for k in range(4) if i + j + k],
    key=lambda o: -sum(min(d, 4 - d) for d in o),
)
CHUNKS = 4
WIDE = 2048 // CHUNKS
ORDER = [4 * place + c for c in range(CHUNKS) for place in range(4)]
BOUNDS = (0, 2, 6, 10, 14, 16)
STEPS = tuple(zip(BOUNDS[:-1], BOUNDS[1:]))
LANES = 128


def block_of(p):
    return slice(ORDER[p] * LANES, (ORDER[p] + 1) * LANES)


def taken_columns(ref, low, high):
    return jnp.concatenate([ref[:, block_of(p)] for p in range(low, high)], axis=1)


def taken_rows(ref, low, high):
    return jnp.concatenate([ref[block_of(p), :] for p in range(low, high)], axis=0)


def mid_part(low, high):
    return slice(2 * low * LANES, (low + high) * LANES)


def cot_part_of(low, high):
    return slice((low + high) * LANES, 2 * high * LANES)


def both_parts(low, high):
    return slice(2 * low * LANES, 2 * high * LANES)


def cot_block(p):
    low, high = [step for step in STEPS if step[0] <= p < step[1]][0]
    at = low + high + p - low
    return slice(at * LANES, (at + 1) * LANES)


def layer_kernel(
    experts_ref,
    weights_ref,
    mid_hbm,
    cot_hbm,
    gate_hbm,
    up_hbm,
    down_hbm,
    out_w_hbm,
    q_hbm,
    k_hbm,
    v_hbm,
    decay_hbm,
    gate_out,
    up_out,
    down_out,
    out_out,
    q_out,
    k_out,
    v_out,
    decay_out,
    mid_ref,
    cot_ref,
    gate_w,
    up_w,
    down_w,
    out_w,
    q_ref,
    k_ref,
    v_ref,
    decay_ref,
    z_send,
    z_note_send,
    z_recv,
    z_note,
    x_send,
    rows,
    pre_gate,
    pre_up,
    back_hidden,
    hidden,
    back_gate,
    back_up,
    half_send,
    half_recv,
    ret_send,
    ret_recv,
    tok_send,
    tok_recv,
    token_all,
    run_log,
    q_near,
    k_near,
    q_start,
    k_end,
    scores,
    normed,
    root,
    s_local,
    s_send,
    s_recv,
    s_back,
    s_in,
    d_send,
    d_recv,
    d_factor,
    n_all,
    b_send,
    b_recv,
    b_back,
    f_in,
    tz,
    o_send,
    o_recv,
    o_part,
    o_last,
    p_send,
    p_recv,
    p_part,
    p_last,
    w_sem,
    n_sem,
    z_sem,
    x_sem,
    d_sem,
    h_sem,
    r_sem,
    t_sem,
    a_sem,
    s_sem,
    e_sem,
    i_sem,
    b_sem,
    f_sem,
    nz_sem,
    tz_sem,
    tz2_sem,
    tz3_sem,
    o_sem,
    o2_sem,
    p_sem,
    p2_sem,
):
    z, y, x, tp = [lax.axis_index(a) for a in SP_TP]
    other = 1 - tp
    here = y * 4 + x
    me = z * 16 + here
    mine = tp * 256

    def z_peer(dz):
        return (ring(z, dz), y, x, tp)

    def plane_peer(dy, dx):
        return (z, ring(y, dy), ring(x, dx), tp)

    partner = (z, y, x, other)
    barrier = pltpu.get_barrier_semaphore()
    peers = [z_peer(dz) for dz in (2, 1, 3)] + [plane_peer(*o) for o in PLANE] + [partner]
    for peer in peers:
        pl.semaphore_signal(barrier, inc=1, device_id=peer, device_id_type=MESH)

    loads = []
    moved = (
        (mid_hbm, mid_ref),
        (cot_hbm, cot_ref),
        (decay_hbm, decay_ref),
        (k_hbm, k_ref),
        (v_hbm, v_ref),
        (q_hbm, q_ref),
        (gate_hbm.at[0], gate_w),
        (up_hbm.at[0], up_w),
        (down_hbm.at[0], down_w),
        (out_w_hbm, out_w),
    )
    for n, (src, dst) in enumerate(moved):
        load = pltpu.make_async_copy(src, dst, w_sem.at[n])
        load.start()
        loads.append(load)

    def remote(src, dst, sem, peer):
        copy = pltpu.make_async_remote_copy(
            src_ref=src,
            dst_ref=dst,
            send_sem=sem.at[0],
            recv_sem=sem.at[1],
            device_id=peer,
            device_id_type=MESH,
        )
        copy.start()

    def settle(ref, sem, side):
        pltpu.make_async_copy(ref, ref, sem.at[side]).wait()

    first = experts_ref[0:1, :]
    second = experts_ref[1:2, :]
    expert_row = lax.broadcasted_iota(jnp.int32, (64, 64), 0)
    token_lane = lax.broadcasted_iota(jnp.int32, (64, 64), 1)
    named_first = ones_where(expert_row == first)
    named_second = ones_where(expert_row == second)
    before = bf(ones_where(expert_row < token_lane))
    counts = dot(bf(named_first + named_second), before)
    rank_first = jnp.sum(named_first * counts, axis=0, keepdims=True)
    rank_second = jnp.sum(named_second * counts, axis=0, keepdims=True)
    group = lax.shift_right_logical(first, 4)
    in_group = ones_where(expert_row[:16] == group)
    group_rank = jnp.sum(in_group * dot(bf(in_group), before), axis=0, keepdims=True)
    z_slot = group * 32 + group_rank.astype(jnp.int32)
    slot_row = lax.broadcasted_iota(jnp.int32, (128, 64), 0)
    z_pick = bf(ones_where(slot_row == z_slot))
    slot_first = (jnp.bitwise_and(first, 15) * 16).astype(jnp.float32) + rank_first
    slot_second = (jnp.bitwise_and(second, 15) * 16).astype(jnp.float32) + rank_second
    columns = [slot_first, slot_second]
    columns += list(pieces_of(weights_ref[0:1, :])) + list(pieces_of(weights_ref[1:2, :]))
    note = ones_where(slot_row == 8)
    for n, column in enumerate(columns):
        note = jnp.where(slot_row == n, column, note)
    z_note_send[...] = bf(dot_cols(z_pick, bf(note)))
    own_z = rows_at(z * 32, 32)
    own_x = rows_at(here * 16, 16)

    loads[0].wait()
    loads[1].wait()

    def fill_z(n):
        z_send[:, mid_part(*STEPS[n])] = bf(dot(z_pick, taken_columns(mid_ref, *STEPS[n])))
        z_send[:, cot_part_of(*STEPS[n])] = bf(dot(z_pick, taken_columns(cot_ref, *STEPS[n])))

    fill_z(0)
    pl.semaphore_wait(barrier, len(peers))

    for dz in (2, 1, 3):
        there = rows_at(ring(z, dz) * 32, 32)
        remote(z_note_send.at[there], z_note.at[own_z], n_sem, z_peer(dz))
    z_note[own_z, :] = z_note_send[own_z, :]

    def send_z(n):
        part = both_parts(*STEPS[n])
        for dz in (2, 1, 3):
            there = rows_at(ring(z, dz) * 32, 32)
            remote(z_send.at[there, part], z_recv.at[own_z, part], z_sem.at[n], z_peer(dz))
        z_recv[own_z, part] = z_send[own_z, part]

    send_z(0)
    fill_z(1)
    send_z(1)

    along_z, along_y, along_x = [[ring(a, d) for d in range(4)] for a in (z, y, x)]
    bases = [[along_z[i] * 16 + along_y[j] * 4 for j in range(4)] for i in range(4)]

    def all_to_all(send):
        for i, j, k in FAR:
            peer = (along_z[i], along_y[j], along_x[k], tp)
            send(peer, bases[i][j] + along_x[k])

    def state_out(peer, there):
        remote(s_send.at[rows_at(there * 16, 16)], s_recv.at[me], s_sem, peer)
        remote(d_send.at[there // 16], d_recv.at[me], e_sem, peer)

    def state_in(peer, there):
        remote(s_back.at[there], s_in.at[own_state], i_sem, peer)

    def grad_out(peer, there):
        remote(b_send.at[rows_at(there * 16, 16)], b_recv.at[me], b_sem, peer)

    def grad_in(peer, there):
        remote(b_back.at[there], f_in.at[own_state], f_sem, peer)

    def scan(recv, back, reverse):
        state = jnp.zeros((16, DK), jnp.float32)
        for n in range(64):
            at = 63 - n if reverse else n
            back[at] = bf(state)
            state = d_factor[at] * state + recv[at].astype(jnp.float32)

    own_state = rows_at(me * 16, 16)
    square = (128, 128)
    at_row = lax.broadcasted_iota(jnp.int32, square, 0)
    at_col = lax.broadcasted_iota(jnp.int32, square, 1)
    upto = at_row >= at_col
    lower = bf(ones_where(upto))
    upper = bf(ones_where(at_row <= at_col))
    for load in loads[2:6]:
        load.wait()
    high, mid, low = pieces_of(decay_ref[...])
    run_log[...] = dot(lower, bf(high)) + dot(lower, bf(mid)) + dot(lower, bf(low))
    for h in range(4):
        ks = slice(h * DK, (h + 1) * DK)
        vs = slice(h * DV, (h + 1) * DV)
        running = run_log[:, ks]
        total = running[127:128]
        d_send[h] = total
        k_end[:, ks] = k_ref[:, ks].astype(jnp.float32) * jnp.exp(total - running)
        k_high, k_low = split(k_end[:, ks])
        state = dot_rows(v_ref[:, vs], k_high) + dot_rows(v_ref[:, vs], k_low)
        s_local[vs, :] = state
        s_send[vs, :] = bf(state)

    settle(z_note.at[0:96], n_sem, 1)
    all_to_all(state_out)
    s_recv[me] = s_send[own_state, :]
    d_recv[me] = d_send[me // 16]
    for n in range(2, len(STEPS)):
        fill_z(n)
        send_z(n)
    got = z_note[...].astype(jnp.float32)
    token_row = lax.broadcasted_iota(jnp.int32, (128, 1), 0)
    offset = lax.shift_right_logical(token_row, 5) * 4
    live = got[:, 8:9] > 0.5
    slot_a = jnp.where(live, got[:, 0:1].astype(jnp.int32) + offset, -1)
    slot_b = jnp.where(live, got[:, 1:2].astype(jnp.int32) + offset, -1)
    slot_lane = lax.broadcasted_iota(jnp.int32, (128, 256), 1)
    place_a = bf(ones_where(slot_lane == slot_a))
    place_b = bf(ones_where(slot_lane == slot_b))
    place = place_a + place_b
    weight_a = got[:, 2:3] + got[:, 3:4] + got[:, 4:5]
    weight_b = got[:, 5:6] + got[:, 6:7] + got[:, 7:8]

    for c, step in enumerate(STEPS):
        settle(z_recv.at[0:96, both_parts(*step)], z_sem.at[c], 1)
        x_send[:, mid_part(*step)] = bf(dot_rows(place, z_recv[:, mid_part(*step)]))
        cot_part = z_recv[:, cot_part_of(*step)].astype(jnp.float32)
        x_send[:, cot_part_of(*step)] = bf(
            dot_rows(place_a, bf(weight_a * cot_part)) + dot_rows(place_b, bf(weight_b * cot_part))
        )
        part = both_parts(*step)
        for dy, dx in PLANE:
            there = rows_at((ring(y, dy) * 4 + ring(x, dx)) * 16, 16)
            remote(
                x_send.at[there, part],
                rows.at[rows_at(mine + here * 16, 16), part],
                x_sem.at[c],
                plane_peer(dy, dx),
            )
        rows[rows_at(mine + here * 16, 16), part] = x_send[own_x, part]
        if c == 1:
            settle(s_recv.at[0:63], s_sem, 1)
            settle(d_recv.at[0:63], e_sem, 1)
            d_factor[...] = jnp.exp(d_recv[...])
            scan(s_recv, s_back, False)
            all_to_all(state_in)
            s_in[own_state, :] = s_back[me]

    for h in range(4):
        ks = slice(h * DK, (h + 1) * DK)
        running = run_log[:, ks]
        middle = running[63:64]
        q_scaled = q_ref[:, ks].astype(jnp.float32) * DK ** (-0.5)
        q_near[:, ks] = q_scaled * jnp.exp(running - middle)
        k_near[:, ks] = k_ref[:, ks].astype(jnp.float32) * jnp.exp(middle - running)
        q_start[:, ks] = q_scaled * jnp.exp(running)
        scores[h] = jnp.where(upto, thrice(dot_cols, q_near[:, ks], k_near[:, ks]), 0.0)
    settle(s_in.at[0:1008], i_sem, 1)
    for h in range(4):
        ks = slice(h * DK, (h + 1) * DK)
        vs = slice(h * DV, (h + 1) * DV)
        raw = twice(dot, scores[h], v_ref[:, vs]) + twice(dot_cols, q_start[:, ks], s_in[vs, :])
        inverse = lax.rsqrt(jnp.mean(raw * raw, axis=-1, keepdims=True) + epsilon)
        normed[:, vs] = raw * inverse
        root[:, h : h + 1] = inverse
        n_all[rows_at(z * 128, 128), vs] = bf(raw * inverse)
    own_n = n_all.at[rows_at(z * 128, 128)]
    for dz in (2, 1, 3):
        remote(own_n, own_n, nz_sem, z_peer(dz))

    for load in loads[6:]:
        load.wait()
    their_rows = rows_at(other * 256, 256)
    own_rows = rows_at(mine, 256)

    def gather_up(c, part):
        step = STEPS[c]
        mid_rows = rows[part, mid_part(*step)]
        for ref, value in (
            (pre_gate, dot(mid_rows, taken_rows(gate_w, *step))),
            (pre_up, dot(mid_rows, taken_rows(up_w, *step))),
            (back_hidden, dot_cols(rows[part, cot_part_of(*step)], taken_columns(down_w, *step))),
        ):
            ref[part, :] = value if c == 0 else ref[part, :] + value

    for c, step in enumerate(STEPS):
        part = both_parts(*step)
        settle(rows.at[0:240, part], x_sem.at[c], 1)
        remote(rows.at[own_rows, part], rows.at[own_rows, part], d_sem.at[c], partner)
        gather_up(c, own_rows)
        settle(rows.at[0:256, part], d_sem.at[c], 1)
        gather_up(c, their_rows)

    gate_swish, gate_slope = silu_parts(pre_gate[...])
    hidden[...] = bf(gate_swish * pre_up[...])
    back_gate[...] = bf(back_hidden[...] * pre_up[...] * gate_slope)
    back_up[...] = bf(back_hidden[...] * gate_swish)

    def half_of(part, c):
        return bf(
            dot_cols(back_gate[part, :], taken_rows(gate_w, 4 * c, 4 * c + 4))
            + dot_cols(back_up[part, :], taken_rows(up_w, 4 * c, 4 * c + 4))
        )

    def send_half(c):
        half_send[c] = half_of(their_rows, c)
        remote(half_send.at[c], half_recv.at[c], h_sem.at[c], partner)

    def give_back(c):
        own_half = half_of(own_rows, c).astype(jnp.float32)
        settle(half_recv.at[c], h_sem.at[c], 1)
        ret_send[c] = bf(own_half + half_recv[c].astype(jnp.float32))
        for dy, dx in PLANE:
            there = rows_at((ring(y, dy) * 4 + ring(x, dx)) * 16, 16)
            remote(ret_send.at[c, there], ret_recv.at[c, own_x], r_sem.at[c], plane_peer(dy, dx))
        ret_recv[c, own_x, :] = ret_send[c, own_x, :]

    send_half(0)
    for c in range(CHUNKS):
        if c + 1 < CHUNKS:
            send_half(c + 1)
        give_back(c)

    for low, high in STEPS:
        mid_rows = rows[:, mid_part(low, high)]
        for out, grad in ((gate_out, back_gate), (up_out, back_up)):
            value = bf(dot_rows(mid_rows, grad[...]))
            for p in range(low, high):
                out[0, block_of(p), :] = value[(p - low) * LANES : (p - low + 1) * LANES, :]
        value = bf(dot_rows(hidden[...], rows[:, cot_part_of(low, high)]))
        for p in range(low, high):
            down_out[0, :, block_of(p)] = value[:, (p - low) * LANES : (p - low + 1) * LANES]

    own_tokens = rows_at(tp * 64, 64)

    def to_tokens(c):
        settle(ret_recv.at[c, 0:240], r_sem.at[c], 1)
        cot_rows = jnp.concatenate(
            [z_recv[:, cot_block(p)] for p in range(4 * c, 4 * c + 4)], axis=1
        )
        tok_send[c] = bf(cot_rows.astype(jnp.float32) + dot(place, ret_recv[c]))
        for dz in (2, 1, 3):
            there = rows_at(ring(z, dz) * 32, 32)
            remote(tok_send.at[c, there], tok_recv.at[c, own_z], t_sem.at[c], z_peer(dz))
        tok_recv[c, own_z, :] = tok_send[c, own_z, :]

    def share_tokens(c):
        settle(tok_recv.at[c, 0:96], t_sem.at[c], 1)
        token_all[c, own_tokens, :] = bf(dot_rows(z_pick, tok_recv[c]))
        part = token_all.at[c, own_tokens]
        remote(part, part, a_sem.at[c], partner)
        last = c == CHUNKS - 1
        for d in (2, 1, 3):
            for core in (tp, other) if last else (tp,):
                remote(
                    token_all.at[c, own_tokens, rows_at(along_z[d] * LANES, LANES)],
                    tz.at[rows_at(z * 128 + tp * 64, 64), c * LANES : (c + 1) * LANES],
                    tz3_sem if last else tz_sem,
                    (along_z[d], y, x, core),
                )

    def use_tokens(c, total):
        settle(token_all.at[c, 0:64], a_sem.at[c], 1)
        value = dot(token_all[c], taken_rows(out_w, 4 * c, 4 * c + 4))
        return value if total is None else total + value

    to_tokens(0)
    to_tokens(1)
    share_tokens(0)
    to_tokens(2)
    share_tokens(1)
    to_tokens(3)
    share_tokens(2)
    back_normed = use_tokens(0, None)
    back_normed = use_tokens(1, back_normed)
    share_tokens(3)
    back_normed = use_tokens(2, back_normed)
    settle(tz.at[0:192, 0:384], tz_sem, 1)
    for d in (1, 2, 3):
        part = tz.at[rows_at(along_z[d] * 128 + tp * 64, 64), 0:384]
        remote(part, part, tz2_sem, partner)
    back_normed = use_tokens(3, back_normed)

    for h in range(4):
        ks = slice(h * DK, (h + 1) * DK)
        vs = slice(h * DV, (h + 1) * DV)
        back = back_normed[:, vs]
        head_normed = normed[:, vs]
        back = root[:, h : h + 1] * (
            back - head_normed * jnp.mean(back * head_normed, axis=-1, keepdims=True)
        )
        normed[:, vs] = back
        b_send[vs, :] = bf(thrice(dot_rows, back, q_start[:, ks]))
    all_to_all(grad_out)
    b_recv[me] = b_send[own_state, :]

    for c in range(CHUNKS):
        tz[rows_at(z * 128, 128), c * LANES : (c + 1) * LANES] = token_all[
            c, :, rows_at(z * LANES, LANES)
        ]
    settle(tz.at[0:192, 0:384], tz2_sem, 1)
    settle(tz.at[0:384, 384:512], tz3_sem, 1)
    settle(n_all.at[0:384], nz_sem, 1)
    o_send[...] = bf(dot_rows(tz[...], n_all[:, :512]))
    for d in (2, 1, 3):
        there = rows_at(along_y[d] * 128, 128)
        remote(o_send.at[there], o_recv.at[y], o_sem, (z, along_y[d], x, tp))
    o_recv[y] = o_send[rows_at(y * 128, 128), :]
    p_send[...] = bf(dot_rows(tz[...], n_all[:, 512:]))
    for d in (2, 1, 3):
        for j in range(4):
            there = rows_at(along_x[d] * 32 + j * 128, 32)
            remote(
                p_send.at[there], p_recv.at[x, j * 32 : (j + 1) * 32], p_sem, (z, y, along_x[d], tp)
            )
    for j in range(4):
        p_recv[x, j * 32 : (j + 1) * 32, :] = p_send[rows_at(x * 32 + j * 128, 32), :]
    settle(b_recv.at[0:63], b_sem, 1)
    scan(b_recv, b_back, True)
    all_to_all(grad_in)
    f_in[own_state, :] = b_back[me]

    for h in range(4):
        ks = slice(h * DK, (h + 1) * DK)
        vs = slice(h * DV, (h + 1) * DV)
        back = normed[:, vs]
        running = run_log[:, ks]
        middle = running[63:64]
        dots = jnp.where(upto, twice(dot_cols, back, v_ref[:, vs]), 0.0)
        q_back = jnp.exp(running - middle) * thrice(dot, dots, k_near[:, ks])
        q_back = q_back + jnp.exp(running) * twice(dot, back, s_in[vs, :])
        k_near[:, ks] = jnp.exp(middle - running) * thrice(dot_rows, dots, q_near[:, ks])
        normed[:, vs] = thrice(dot_rows, scores[h], back)
        q_near[:, ks] = q_back
        q_out[:, ks] = bf(q_back * DK ** (-0.5))
        s_local[vs, :] = jnp.exp(running[127:128]) * s_in[vs, :].astype(jnp.float32) + s_local[vs, :]

    settle(o_recv.at[0:3], o_sem, 1)
    o_part[...] = bf(total_of(o_recv))
    for d in (2, 1, 3):
        there = rows_at(along_x[d] * 32, 32)
        remote(o_part.at[there], o_last.at[x], o2_sem, (z, y, along_x[d], tp))
    o_last[x] = o_part[rows_at(x * 32, 32), :]
    settle(p_recv.at[0:3], p_sem, 1)
    p_part[...] = bf(total_of(p_recv))
    for d in (2, 1, 3):
        there = rows_at(along_y[d] * 32, 32)
        remote(p_part.at[there], p_last.at[y], p2_sem, (z, along_y[d], x, tp))
    p_last[y] = p_part[rows_at(y * 32, 32), :]
    settle(z_note_send.at[0:96], n_sem, 0)
    settle(s_send.at[0:1008], s_sem, 0)
    settle(d_recv.at[0:63], e_sem, 0)
    settle(s_back.at[0:63], i_sem, 0)
    settle(n_all.at[0:384], nz_sem, 0)
    settle(tz.at[0:192, 0:384], tz_sem, 0)
    settle(tz.at[0:192, 0:384], tz2_sem, 0)
    settle(tz.at[0:384, 384:512], tz3_sem, 0)
    settle(b_send.at[0:1008], b_sem, 0)
    for c, step in enumerate(STEPS):
        settle(z_send.at[0:96, both_parts(*step)], z_sem.at[c], 0)
        settle(x_send.at[0:240, both_parts(*step)], x_sem.at[c], 0)
        settle(rows.at[0:256, both_parts(*step)], d_sem.at[c], 0)
    for c in range(CHUNKS):
        settle(half_send.at[c], h_sem.at[c], 0)
        settle(ret_send.at[c, 0:240], r_sem.at[c], 0)
        settle(tok_send.at[c, 0:96], t_sem.at[c], 0)
        settle(token_all.at[c, 0:64], a_sem.at[c], 0)
    settle(f_in.at[0:1008], f_sem, 1)
    for h in range(4):
        ks = slice(h * DK, (h + 1) * DK)
        vs = slice(h * DV, (h + 1) * DV)
        running = run_log[:, ks]
        total = running[127:128]
        future = f_in[vs, :]
        k_back = k_near[:, ks] + jnp.exp(total - running) * dot(v_ref[:, vs], future)
        k_out[:, ks] = bf(k_back)
        v_out[:, vs] = bf(normed[:, vs] + twice(dot_cols, k_end[:, ks], future))
        cross = jnp.sum(s_local[vs, :] * future.astype(jnp.float32), axis=0, keepdims=True)
        q_scaled = q_ref[:, ks].astype(jnp.float32) * DK ** (-0.5)
        change = q_scaled * q_near[:, ks] - k_ref[:, ks].astype(jnp.float32) * k_back
        high, mid, low = pieces_of(change)
        within = dot(upper, bf(high)) + dot(upper, bf(mid)) + dot(upper, bf(low))
        decay_out[:, ks] = within + cross

    settle(o_last.at[0:3], o2_sem, 1)
    settle(p_last.at[0:3], p2_sem, 1)
    out_out[:, :512] = total_of(o_last)
    out_out[:, 512:] = total_of(p_last)
    settle(o_recv.at[0:3], o_sem, 0)
    settle(p_recv.at[0:3], p_sem, 0)
    settle(o_last.at[0:3], o2_sem, 0)
    settle(p_last.at[0:3], p2_sem, 0)
    settle(b_back.at[0:63], f_sem, 0)


def finish_kernel(*refs):
    count = len(refs) // 2
    sems = refs[-1]
    copies = []
    for n in range(count):
        copy = pltpu.make_async_copy(refs[n], refs[count + n], sems.at[n])
        copy.start()
        copies.append(copy)
    for copy in copies:
        copy.wait()


def whole_layer(experts, weights, mid, cot, gate, up, down, out_w, queries, keys, values, decay):
    b16, f32 = jnp.bfloat16, jnp.float32
    v = pltpu.VMEM
    dma = pltpu.SemaphoreType.DMA
    vmem = pl.BlockSpec(memory_space=pltpu.VMEM)
    hbm = pl.BlockSpec(memory_space=pl.ANY)
    outs = (
        ((1, 2048, 512), b16),
        ((1, 2048, 512), b16),
        ((1, 512, 2048), b16),
        ((32, 1024), f32),
        ((128, 512), b16),
        ((128, 512), b16),
        ((128, 1024), b16),
        ((128, 512), f32),
    )
    scratch = (
        ((64, 2048), b16),
        ((64, 2048), b16),
        ((2048, 512), b16),
        ((2048, 512), b16),
        ((512, 2048), b16),
        ((2048, 1024), b16),
        ((128, 512), b16),
        ((128, 512), b16),
        ((128, 1024), b16),
        ((128, 512), f32),
        ((128, 4096), b16),
        ((128, 128), b16),
        ((128, 4096), b16),
        ((128, 128), b16),
        ((256, 4096), b16),
        ((512, 4096), b16),
        ((512, 512), f32),
        ((512, 512), f32),
        ((512, 512), f32),
        ((512, 512), b16),
        ((512, 512), b16),
        ((512, 512), b16),
        ((CHUNKS, 256, WIDE), b16),
        ((CHUNKS, 256, WIDE), b16),
        ((CHUNKS, 256, WIDE), b16),
        ((CHUNKS, 256, WIDE), b16),
        ((CHUNKS, 128, WIDE), b16),
        ((CHUNKS, 128, WIDE), b16),
        ((4, 128, 512), b16),
        ((128, 512), f32),
        ((128, 512), f32),
        ((128, 512), f32),
        ((128, 512), f32),
        ((128, 512), f32),
        ((4, 128, 128), f32),
        ((128, 1024), f32),
        ((128, 128), f32),
        ((1024, 128), f32),
        ((1024, 128), b16),
        ((64, 16, 128), b16),
        ((64, 16, 128), b16),
        ((1024, 128), b16),
        ((4, 1, 128), f32),
        ((64, 1, 128), f32),
        ((64, 1, 128), f32),
        ((512, 1024), b16),
        ((1024, 128), b16),
        ((64, 16, 128), b16),
        ((64, 16, 128), b16),
        ((1024, 128), b16),
        ((512, 512), b16),
        ((512, 512), b16),
        ((4, 128, 512), b16),
        ((128, 512), b16),
        ((4, 32, 512), b16),
        ((512, 512), b16),
        ((4, 128, 512), b16),
        ((128, 512), b16),
        ((4, 32, 512), b16),
    )
    two, many, steps = (2,), (CHUNKS, 2), (len(STEPS), 2)
    sems = [(10,), two] + [steps] * 3 + [many] * 4 + [two] * 13
    made = pl.pallas_call(
        layer_kernel,
        name="whole_layer",
        out_shape=tuple(v(shape, kind) for shape, kind in outs),
        in_specs=[vmem] * 2 + [hbm] * 10,
        out_specs=(vmem,) * 8,
        scratch_shapes=[v(shape, kind) for shape, kind in scratch] + [dma(shape) for shape in sems],
        compiler_params=pltpu.CompilerParams(
            collective_id=0, has_side_effects=True, vmem_limit_bytes=50 * 1024 * 1024
        ),
        cost_estimate=pl.CostEstimate(
            flops=11_000_000_000, bytes_accessed=20_000_000, transcendentals=600_000
        ),
    )(experts.T, weights.T, mid, cot, gate, up, down, out_w, queries, keys, values, decay)
    return pl.pallas_call(
        finish_kernel,
        name="finish",
        out_shape=tuple(jax.ShapeDtypeStruct(shape, kind) for shape, kind in outs),
        in_specs=[vmem] * 8,
        out_specs=(hbm,) * 8,
        scratch_shapes=[dma((8,))],
        compiler_params=pltpu.CompilerParams(vmem_limit_bytes=1024 * 1024),
    )(*[pltpu.with_memory_space_constraint(a, pltpu.VMEM) for a in made])


def body(
    mid_rows,
    cotangent,
    route_experts,
    route_weights,
    gate_weight,
    up_weight,
    down_weight,
    out_weight,
    queries,
    key_rows,
    value_rows,
    log_decay,
):
    return whole_layer(
        route_experts,
        route_weights,
        mid_rows,
        cotangent,
        gate_weight,
        up_weight,
        down_weight,
        out_weight,
        queries,
        key_rows,
        value_rows,
        log_decay,
    )


def solution(mesh):
    split = Mesh(mesh.devices.reshape(4, 4, 4, mesh.shape["tp"]), ("sp_0", "sp_1", "sp_2", "tp"))
    placed = (
        P(SP_TP, None),
        P(SP_TP, None),
        P(SP_TP, None),
        P(SP_TP, None),
        P(SP, None, "tp"),
        P(SP, None, "tp"),
        P(SP, "tp", None),
        P(None, "tp"),
        P(SP, "tp"),
        P(SP, "tp"),
        P(SP, "tp"),
        P(SP, "tp"),
    )
    return jax.shard_map(
        body,
        mesh=split,
        in_specs=placed,
        out_specs=(
            P(SP, None, "tp"),
            P(SP, None, "tp"),
            P(SP, "tp", None),
            P(SP, "tp"),
            P(SP, "tp"),
            P(SP, "tp"),
            P(SP, "tp"),
            P(SP, "tp"),
        ),
        check_vma=False,
    )
```
